256 devices in a mesh: ep: 16 (over y, x), tp: 16 (over z, core).
Axes of the slice: x: 4, y: 4, z: 8, core: 2. Of those that a mesh axis runs over, the one named last changes fastest.
Arguments:
- hidden_in: bfloat16 [512, 4096], P('ep'), may hold values from -6 to 6
- mix_gain: float32 [4096], replicated, may hold values from 0.1 to 1.9
- w_query: bfloat16 [4096, 2048], P('ep', 'tp'), may hold values from -0.09375 to 0.09375
- w_key: bfloat16 [4096, 2048], P('ep', 'tp'), may hold values from -0.09375 to 0.09375
- w_value: bfloat16 [4096, 2048], P('ep', 'tp'), may hold values from -0.09375 to 0.09375
- w_outgate: bfloat16 [4096, 2048], P('ep', 'tp'), may hold values from -0.09375 to 0.09375
- w_gates: bfloat16 [2, 4096, 32], P(None, None, 'tp'), may hold values from -0.09375 to 0.09375
- gate_bias: float32 [2, 32], P(None, 'tp'), may hold values from -1 to 4
- state_matrix: float32 [512, 32, 64, 64], P('ep', 'tp'), may hold values from -2 to 2
- state_norm: float32 [512, 32, 64], P('ep', 'tp'), may hold values from -2 to 2
- state_max: float32 [512, 32], P('ep', 'tp'), may hold values from -3 to 3
- w_mix_out: bfloat16 [2048, 4096], P('tp'), may hold values from -0.125 to 0.125
- ffn_gain: float32 [4096], replicated, may hold values from 0.1 to 1.9
- routes: int32 [512, 2], replicated, may hold values from 0 to 31, all different within a row; in each aligned block of 32 rows (0 to 31, 32 to 63, ...) at most 3 rows name the same one
- route_weights: float32 [512, 2], P('ep'), may hold values from 0.1 to 1
- expert_gate: bfloat16 [32, 4096, 2048], P('ep', None, 'tp'), may hold values from -0.09375 to 0.09375
- expert_up: bfloat16 [32, 4096, 2048], P('ep', None, 'tp'), may hold values from -0.09375 to 0.09375
- expert_down: bfloat16 [32, 2048, 4096], P('ep', 'tp'), may hold values from -0.125 to 0.125
- shared_gate: bfloat16 [4096, 1024], P(None, 'tp'), may hold values from -0.09375 to 0.09375
- shared_up: bfloat16 [4096, 1024], P(None, 'tp'), may hold values from -0.09375 to 0.09375
- shared_down: bfloat16 [1024, 4096], P('tp'), may hold values from -0.1875 to 0.1875
Outputs:
- result: bfloat16 [512, 4096], P('ep', 'tp')
- new_matrix: float32 [512, 32, 64, 64], P('ep', 'tp')
- new_norm: float32 [512, 32, 64], P('ep', 'tp')
- new_max: float32 [512, 32], P('ep', 'tp')
The draws below stay inside these ranges and needn't reach their ends.
Inputs may be any that keep to these rules, and one draw needn't show every extreme that they name: `routes`: each row names 2 different experts. In each aligned block of 32 rows (the rows of one device group along ep) no expert is named by more than 3 rows, a bound that some block reaches.
All inputs are finite; a program needn't handle non-finite values.
Results may differ from the reference program's by a relative error of at most 0.023.
Values may be sent and summed in bfloat16 or wider, within the bound.
A program may use at most 64 MiB of HBM per device.

```python
import math
import jax
import jax.numpy as jnp
import numpy as np
from jax import lax

D = 4096
HEADS = 32
HEAD_DIM = 64
EXPERT_WIDTH = 2048
SHARED_WIDTH = 1024
TOP = 2
SEQ_GRP = 32
M_WIDTH = 2048
EXPERTS = 32
CAP = 3
BATCH = 512
N_EP = 16
N_TP = 16


def block_scale(own_key, shape, cuts, least, top_value):
    gain = 1.0
    for axis_at, parts in cuts:
        heights = jax.random.uniform(jax.random.fold_in(jax.random.fold_in(own_key, 6), axis_at), (parts,), jnp.float32, least / len(cuts), top_value / len(cuts))
        gain = gain * jnp.repeat(jnp.exp(heights), shape[axis_at] // parts).reshape((-1,) + (1,) * (len(shape) - 1 - axis_at))
    return gain


def deal_out(key, own, number, rows, count, top, most, skew):
    sequence = jax.random.permutation(key, count)
    packed, ordinary = portions_of(count, rows * top, most, skew, True), portions_of(count, rows * top, most, skew, False)
    places = jnp.arange(count)

    def named(lengths, rotation):
        used = int((lengths > 0).sum())
        fixed = max(1, used // 4)
        shifted = fixed + (places - fixed + rotation * (used - fixed)) % max(1, count - fixed)
        return jnp.zeros((count,), jnp.int32).at[sequence[jnp.where(places < fixed, places, shifted)]].set(jnp.asarray(lengths, jnp.int32))

    lengths = jnp.where(number % 4 == 0, named(packed, number // 4), named(ordinary, number - number // 4 - 1))
    mixed = jax.random.permutation(jax.random.fold_in(own, 3), count)
    source_of, receiver = mixed[0:count // 2 * 2:2], mixed[1:count // 2 * 2:2]
    room = jnp.minimum(lengths[source_of] - 1, most - lengths[receiver]) // 2
    room = jnp.where((source_of == sequence[0]) | (receiver == sequence[0]) | (lengths[receiver] == 0), 0, jnp.maximum(room, 0))
    shifted = jax.random.randint(jax.random.fold_in(own, 4), (count // 2,), 0, 1 << 20) % (room + 1)
    lengths = lengths.at[source_of].add(-shifted).at[receiver].add(shifted)
    items = jnp.searchsorted(jnp.cumsum(lengths), jnp.arange(rows * top), side="right").astype(jnp.int32)
    table = items.reshape(top, rows).T
    table = table[jax.random.permutation(jax.random.fold_in(own, 1), rows)]
    rotation = jax.random.randint(jax.random.fold_in(own, 2), (rows, 1), 0, top)
    return jnp.take_along_axis(table, (jnp.arange(top)[None, :] + rotation) % top, axis=1)


def portions_of(number_of, total, reach, lean, full):
    portions = [(1 << 20) // math.isqrt(standing ** lean) + 1 for standing in range(1, number_of + 1)]
    largest = reach if full else min(reach, max(-(-total // number_of), total * portions[0] // sum(portions)))
    least = 1 if total - largest >= number_of - 1 else 0
    holding, surplus = [largest] + [least] * (number_of - 1), total - largest - least * (number_of - 1)
    while surplus > 0:
        movable = [i for i in range(1, number_of) if holding[i] < largest] or [i for i in range(1, number_of) if holding[i] < reach]
        pool, left = sum([portions[i] for i in movable]), surplus
        for i in movable:
            addition = min(reach - holding[i], max(1, left * portions[i] // pool), surplus)
            holding[i] = holding[i] + addition
            surplus = surplus - addition
    return np.array(holding)


def bell_draw(rng, extent, scale, reach, cuts=(), kind=jnp.bfloat16):
    level = block_scale(rng, extent, cuts, -0.22, 0.18) if cuts else 1.0
    values = jax.random.normal(rng, extent, jnp.float32) * scale * level
    return jnp.minimum(jnp.maximum(values, -reach), reach).astype(kind)


def setup_inputs(seed: int = 0) -> dict:
    streams_of = jax.random.split(jax.random.key(seed), 22)
    hidden_in = bell_draw(streams_of[0], (BATCH, D), 1.0, 6.0, ((0, 16),))
    mix_gain = jnp.clip(1.0 + 0.18 * jax.random.normal(streams_of[1], (D,), jnp.float32), 0.1, 1.9)
    w_query = bell_draw(streams_of[2], (D, M_WIDTH), D ** -0.5, 0.09375, ((0, 16), (1, 16)))
    w_key = bell_draw(streams_of[3], (D, M_WIDTH), D ** -0.5, 0.09375, ((0, 16), (1, 16)))
    w_value = bell_draw(streams_of[4], (D, M_WIDTH), D ** -0.5, 0.09375, ((0, 16), (1, 16)))
    w_outgate = bell_draw(streams_of[5], (D, M_WIDTH), D ** -0.5, 0.09375, ((0, 16), (1, 16)))
    w_gates = bell_draw(streams_of[6], (2, D, HEADS), D ** -0.5, 0.09375, ((2, 16),))
    gate_bias = jnp.clip(-1.0 + 5.0 * jax.random.uniform(streams_of[7], (2, HEADS), jnp.float32) ** block_scale(streams_of[7], (2, HEADS), ((1, 16),), -0.2, 0.2), -1.0, 4.0)
    state_matrix = bell_draw(streams_of[8], (BATCH, HEADS, HEAD_DIM, HEAD_DIM), 0.15, 2.0, ((0, 16), (1, 16)), jnp.float32)
    state_norm = bell_draw(streams_of[9], (BATCH, HEADS, HEAD_DIM), 0.15, 2.0, ((0, 16), (1, 16)), jnp.float32)
    state_max = jnp.clip(jax.random.uniform(streams_of[10], (BATCH, HEADS), jnp.float32, -3.0, 3.0) * block_scale(streams_of[10], (BATCH, HEADS), ((0, 16), (1, 16)), -0.4, 0.0), -3.0, 3.0)
    w_mix_out = bell_draw(streams_of[11], (M_WIDTH, D), M_WIDTH ** -0.5, 0.125, ((0, 16),))
    ffn_gain = jnp.clip(1.0 + 0.18 * jax.random.normal(streams_of[12], (D,), jnp.float32), 0.1, 1.9)
    routes_keys = jax.random.split(jax.random.fold_in(streams_of[13], 1), BATCH // SEQ_GRP)
    routes_turns = jax.random.permutation(jax.random.fold_in(streams_of[13], 3), BATCH // SEQ_GRP)
    routes = jax.vmap(lambda own, number: deal_out(jax.random.fold_in(streams_of[13], 2), own, number, SEQ_GRP, EXPERTS, TOP, CAP, 2))(routes_keys, routes_turns).reshape((BATCH, TOP))
    route_weights = jnp.clip(jnp.exp(math.log(1.0) - 2.3025851 * jax.random.uniform(streams_of[14], (BATCH, TOP), jnp.float32) ** block_scale(streams_of[14], (BATCH, TOP), ((0, 16),), -0.2, 0.2)), 0.1, 1.0)
    expert_gate = bell_draw(streams_of[15], (EXPERTS, D, EXPERT_WIDTH), D ** -0.5, 0.09375, ((0, 16), (2, 16)))
    expert_up = bell_draw(streams_of[16], (EXPERTS, D, EXPERT_WIDTH), D ** -0.5, 0.09375, ((0, 16), (2, 16)))
    expert_down = bell_draw(streams_of[17], (EXPERTS, EXPERT_WIDTH, D), EXPERT_WIDTH ** -0.5, 0.125, ((0, 16), (1, 16)))
    shared_gate = bell_draw(streams_of[18], (D, SHARED_WIDTH), D ** -0.5, 0.09375, ((1, 16),))
    shared_up = bell_draw(streams_of[19], (D, SHARED_WIDTH), D ** -0.5, 0.09375, ((1, 16),))
    shared_down = bell_draw(streams_of[20], (SHARED_WIDTH, D), SHARED_WIDTH ** -0.5, 0.1875, ((0, 16),))
    return dict(hidden_in=hidden_in, mix_gain=mix_gain, w_query=w_query, w_key=w_key, w_value=w_value, w_outgate=w_outgate, w_gates=w_gates, gate_bias=gate_bias, state_matrix=state_matrix, state_norm=state_norm, state_max=state_max, w_mix_out=w_mix_out, ffn_gain=ffn_gain, routes=routes, route_weights=route_weights, expert_gate=expert_gate, expert_up=expert_up, expert_down=expert_down, shared_gate=shared_gate, shared_up=shared_up, shared_down=shared_down)


norm_eps = 1e-06

def rms_scale(inputs, scales):
    floats = inputs.astype(jnp.float32)
    return floats * lax.rsqrt(lax.optimization_barrier(jnp.mean(floats * floats, -1, keepdims=True)) + norm_eps) * scales

def block_sum(hidden, down_weight):
    row_count = hidden.shape[0]
    unit_count = hidden.shape[1]
    hidden_blocks = hidden.astype(jnp.float32).reshape(row_count, N_TP, unit_count // N_TP)
    down_blocks = down_weight.astype(jnp.float32).reshape(N_TP, unit_count // N_TP, down_weight.shape[1])
    partial_value = jnp.einsum('rpf,pfd->prd', hidden_blocks, down_blocks).astype(jnp.bfloat16)
    return lax.optimization_barrier(jnp.sum(partial_value.astype(jnp.float32), 0))

def reference(hidden_in, mix_gain, w_query, w_key, w_value, w_outgate, w_gates, gate_bias, state_matrix, state_norm, state_max, w_mix_out, ffn_gain, routes, route_weights, expert_gate, expert_up, expert_down, shared_gate, shared_up, shared_down):
    normed = rms_scale(hidden_in, mix_gain).astype(jnp.bfloat16)

    def project(weight):
        rounded = jnp.dot(normed, weight, preferred_element_type=jnp.float32).astype(jnp.bfloat16)
        rounded = lax.optimization_barrier(rounded)
        return rounded.astype(jnp.float32).reshape(BATCH, HEADS, HEAD_DIM)
    query_heads = project(w_query)
    key_heads = project(w_key) * HEAD_DIM ** (-0.5)
    value_heads = project(w_value)
    out_gate = project(w_outgate)
    gate_pre = jnp.einsum('sd,gdh->gsh', normed.astype(jnp.float32), w_gates.astype(jnp.float32))
    gate_pre = gate_pre + gate_bias[:, None, :]
    carried = jax.nn.log_sigmoid(gate_pre[1]) + state_max
    new_max = jnp.maximum(carried, gate_pre[0])
    forget_weight = jnp.exp(carried - new_max)[..., None]
    input_weight = jnp.exp(gate_pre[0] - new_max)[..., None]
    new_norm = forget_weight * state_norm + input_weight * key_heads
    new_matrix = forget_weight[..., None] * state_matrix + (input_weight * value_heads)[..., :, None] * key_heads[..., None, :]
    numerator = jnp.einsum('shek,shk->she', new_matrix, query_heads, precision=lax.Precision.HIGHEST)
    denominator = jnp.maximum(jnp.abs(lax.optimization_barrier(jnp.sum(new_norm * query_heads, -1))), 1.0)
    gated_out = (jax.nn.sigmoid(out_gate) * numerator / denominator[..., None]).reshape(BATCH, M_WIDTH)
    gated_out = gated_out.astype(jnp.bfloat16)
    stream = (hidden_in.astype(jnp.float32) + jnp.dot(gated_out, w_mix_out, preferred_element_type=jnp.float32)).astype(jnp.bfloat16)
    ffn_in = rms_scale(stream, ffn_gain).astype(jnp.bfloat16)
    shared_hidden = (jax.nn.silu(jnp.dot(ffn_in, shared_gate, preferred_element_type=jnp.float32)) * jnp.dot(ffn_in, shared_up, preferred_element_type=jnp.float32)).astype(jnp.bfloat16)
    shared_out = block_sum(shared_hidden, shared_down)
    grouped = routes.reshape(N_EP, SEQ_GRP * TOP)
    onehot = (grouped[..., None] == jnp.arange(EXPERTS, dtype=jnp.int32)[None, None, :]).astype(jnp.int32)
    earlier = jnp.cumsum(onehot, 1) - onehot
    rank_counts = lax.optimization_barrier(jnp.sum(earlier * onehot, -1))
    group_ids = jnp.arange(N_EP, dtype=jnp.int32)[:, None]
    slot_ids = (grouped * (N_EP * CAP) + group_ids * CAP + rank_counts).reshape(-1).astype(jnp.int32)
    token_ids = (jnp.arange(BATCH * TOP, dtype=jnp.int32) // TOP).astype(jnp.int32)
    slot_tokens = jnp.full((EXPERTS * N_EP * CAP,), BATCH, jnp.int32).at[slot_ids].set(token_ids)
    padded_in = jnp.concatenate([ffn_in, jnp.zeros((1, D), jnp.bfloat16)], 0)

    def run_expert(operands):
        slot_picks, gate_weight, up_weight, down_weight = operands
        rows_in = padded_in[slot_picks]
        hidden = (jax.nn.silu(jnp.dot(rows_in, gate_weight, preferred_element_type=jnp.float32)) * jnp.dot(rows_in, up_weight, preferred_element_type=jnp.float32)).astype(jnp.bfloat16)
        return block_sum(hidden, down_weight).astype(jnp.bfloat16)
    expert_rows = lax.map(run_expert, (slot_tokens.reshape(EXPERTS, N_EP * CAP), expert_gate, expert_up, expert_down))
    flat_rows = expert_rows.reshape(EXPERTS * N_EP * CAP, D)
    picked = flat_rows[slot_ids].astype(jnp.float32).reshape(BATCH, TOP, D)
    routed = lax.optimization_barrier(jnp.sum(route_weights[..., None] * picked, 1))
    result = (stream.astype(jnp.float32) + shared_out + routed).astype(jnp.bfloat16)
    return (result, new_matrix, new_norm, new_max)
```

```python
import functools

import jax
import jax.numpy as jnp
from jax import lax
from jax.experimental import pallas as pl
from jax.experimental.pallas import tpu as pltpu
from jax.sharding import PartitionSpec as P

MESH = pl.DeviceIdType.MESH
NORM_EPS = 1e-06
ROOM = 4


def remote(src, dst, send_sem, recv_sem, dev):
    return pltpu.make_async_remote_copy(
        src_ref=src, dst_ref=dst, send_sem=send_sem, recv_sem=recv_sem, device_id=dev, device_id_type=MESH
    )


def wait_bytes(ref, sem):
    pltpu.make_async_copy(ref, ref, sem).wait()


def far_first(n):
    return sorted(range(1, n), key=lambda i: (-min(i, n - i), i))


def near_first(n):
    return sorted(range(1, n), key=lambda i: (min(i, n - i), i))


def layer_kernel(
    cfg,
    hidden_h, mgain_h, wq_h, wk_h, wv_h, wo_h, wg_h, bias_s, state_h, snorm_h, smax_h, wmix_h, fgain_h,
    routes_h, rw_h, eg_h, eu_h, ed_h, sg_h, su_h, sd_h,
    result_o, newmat_o, newnorm_o, newmax_o,
    hid, mgain, wqkvo, wg, state, snorm, smax, wmix, fgain, routes, rw, wcat, down, sgu, sdown,
    xn, ga, pt, qa, kvq, nums, gated, mixs, mixr, mixo, rz, so, st, disp, dx, xg, acc, po, pi, ret, rt, shs, shr, sho, fin, fz,
    nnew, mnew, lsem, s1, r1, s2, r2, s3, r3, s4, r4, s5, r5, s6, r6, s7, r7, s8, r8, s9, r9, s10, r10, s11, r11, s12, r12, osem,
):
    EY, EX, Z, S, D, HD, L = cfg
    E, T = EY * EX, 2 * Z
    W = D // T
    f32, bf16 = jnp.float32, jnp.bfloat16
    e, t = lax.axis_index("ep"), lax.axis_index("tp")
    z, c = lax.div(t, 2), lax.rem(t, 2)
    o = 1 - c
    sib = (e, z * 2 + o)
    y, x = lax.div(e, EX), lax.rem(e, EX)

    def ep_peer(i):
        return lax.rem(y + lax.div(i, EX), EY) * EX + lax.rem(x + lax.rem(i, EX), EX)

    def ep_src(i):
        return lax.rem(y + EY - lax.div(i, EX), EY) * EX + lax.rem(x + EX - lax.rem(i, EX), EX)

    def z_dev(zz):
        return (e, zz * 2 + c)

    def zp(i):
        return lax.rem(z + i, Z)

    def zs(i):
        return lax.rem(z + Z - i, Z)

    def col(zz, cc):
        return pl.ds(pl.multiple_of((zz * 2 + cc) * W, W), W)

    def half(zz):
        return pl.ds(pl.multiple_of(zz * W, W), W)

    def rows(g):
        return pl.ds(pl.multiple_of(g * L * ROOM, L * ROOM), L * ROOM)

    loads = []

    def load(src, dst):
        cp = pltpu.make_async_copy(src, dst, lsem.at[len(loads)])
        cp.start()
        loads.append(cp)
        return cp

    ld_hid = load(hidden_h, hid)
    ld_mg = load(mgain_h, mgain)
    ld_w = [load(w, wqkvo.at[:, k * 128 : (k + 1) * 128]) for k, w in enumerate((wq_h, wk_h, wv_h, wo_h))]
    ld_wg = load(wg_h, wg)
    ld_sm = load(smax_h, smax)
    ld_rt = load(routes_h, routes)
    ld_rw = load(rw_h, rw)
    ld_sn = load(snorm_h, snorm)
    ld_st = load(state_h, state)
    ld_mix = load(wmix_h, wmix)
    ld_fg = load(fgain_h, fgain)
    ld_sg = load(sg_h, sgu.at[0 : sg_h.shape[0], :])
    ld_su = load(su_h, sgu.at[sg_h.shape[0] :, :])
    ld_sd = load(sd_h, sdown)
    ld_ed = load(ed_h, down)
    cat_sem = lsem.at[len(loads)]

    def cat_copies(k):
        zz, cc = lax.div(k, 2), lax.rem(k, 2)
        return [
            pltpu.make_async_copy(
                src.at[j, pl.ds(pl.multiple_of(k * W, W), W), :],
                wcat.at[cc, pl.ds(pl.multiple_of(zz * W, W), W), (2 * j + q) * 128 : (2 * j + q + 1) * 128],
                cat_sem,
            )
            for j in range(L)
            for q, src in enumerate((eg_h, eu_h))
        ]

    def start_cat(k, _):
        for cp in cat_copies(k):
            cp.start()
        return 0

    lax.fori_loop(0, T, start_cat, 0)

    barrier = pltpu.get_barrier_semaphore()

    def greet(i, _):
        pl.semaphore_signal(barrier, inc=1, device_id=(ep_peer(i), t), device_id_type=MESH)
        return 0

    lax.fori_loop(1, E, greet, 0)
    for i in range(1, Z):
        pl.semaphore_signal(barrier, inc=1, device_id=z_dev(zp(i)), device_id_type=MESH)
    pl.semaphore_signal(barrier, inc=1, device_id=sib, device_id_type=MESH)

    ld_hid.wait()
    ld_mg.wait()
    KS = D // E
    sq = jnp.zeros((S, 128), f32)
    for k in range(D // 128):
        v = hid[:, k * 128 : (k + 1) * 128].astype(f32)
        sq = sq + v * v
    scale = lax.rsqrt(jnp.sum(sq, -1, keepdims=True) * (1.0 / D) + NORM_EPS)
    for k in range(E):
        v = hid[:, k * KS : (k + 1) * KS].astype(f32)
        xn[k] = (v * scale * mgain[:, k * KS : (k + 1) * KS]).astype(bf16)

    pl.semaphore_wait(barrier, E - 1 + Z - 1 + 1)

    def send_x(i, _):
        p = ep_peer(i)
        remote(xn.at[p], ga.at[e], s1.at[i], r1.at[i], (p, t)).start()
        return 0

    lax.fori_loop(1, E, send_x, 0)

    for cp in ld_w:
        cp.wait()
    qa[0] = jnp.dot(xn[e], wqkvo[...], preferred_element_type=f32).astype(bf16)

    ld_wg.wait()
    ld_sm.wait()
    ld_rt.wait()
    ld_rw.wait()
    HN = 2
    gsum = [[jnp.zeros((S, 128), f32) for _ in range(HN)] for _ in range(2)]
    for k in range(D // 128):
        v = xn[k * 128 // KS, :, (k * 128) % KS : (k * 128) % KS + 128].astype(f32)
        for g in range(2):
            w2 = wg[g, :, k * 128 : (k + 1) * 128].astype(f32)
            for h in range(HN):
                gsum[g][h] = gsum[g][h] + v * w2[h : h + 1, :]
    eye = lax.broadcasted_iota(jnp.int32, (S, S), 0) == lax.broadcasted_iota(jnp.int32, (S, S), 1)
    smax_v = smax[...]
    fws, iws = [], []
    for h in range(HN):
        gi = jnp.sum(gsum[0][h], -1, keepdims=True) + bias_s[0, h]
        gf = jnp.sum(gsum[1][h], -1, keepdims=True) + bias_s[1, h]
        old = jnp.sum(jnp.where(eye, smax_v[h : h + 1, :], 0.0), -1, keepdims=True)
        carried = jnp.minimum(gf, 0.0) - jnp.log(1.0 + jnp.exp(-jnp.abs(gf))) + old
        nm = jnp.maximum(carried, gi)
        fws.append(jnp.exp(carried - nm))
        iws.append(jnp.exp(gi - nm))
        mnew[h : h + 1, :] = jnp.sum(jnp.where(eye, nm, 0.0), 0, keepdims=True)

    GR = routes_h.shape[1]
    sel = (
        lax.broadcasted_iota(jnp.int32, (S, GR), 1) == lax.broadcasted_iota(jnp.int32, (S, GR), 0) + e * S
    )
    all_routes = routes[...].astype(f32)
    sel_f = jnp.where(sel, 1.0, 0.0)
    r_col = [jnp.sum(sel_f * all_routes[j : j + 1, :], -1, keepdims=True) for j in range(2)]
    r_row = [jnp.sum(jnp.where(eye, r_col[j], 0.0), 0, keepdims=True) for j in range(2)]
    i0 = lax.broadcasted_iota(jnp.int32, (S, S), 0)
    i1 = lax.broadcasted_iota(jnp.int32, (S, S), 1)
    NS = E * L * ROOM
    slot_row, slot_col = [], []
    for j in range(2):
        same = jnp.where(r_col[0] == r_row[j], 1.0, 0.0) + jnp.where(r_col[1] == r_row[j], 1.0, 0.0)
        rank_row = jnp.sum(jnp.where(i0 < i1, same, 0.0), 0, keepdims=True)
        slot_row.append(r_row[j] * ROOM + rank_row)
        same = jnp.where(r_row[0] == r_col[j], 1.0, 0.0) + jnp.where(r_row[1] == r_col[j], 1.0, 0.0)
        rank_col = jnp.sum(jnp.where(i1 < i0, same, 0.0), -1, keepdims=True)
        slot_col.append(r_col[j] * ROOM + rank_col)
    slot_ids = lax.broadcasted_iota(jnp.int32, (NS, S), 0).astype(f32)
    chooser = jnp.where((slot_ids == slot_row[0]) | (slot_ids == slot_row[1]), 1.0, 0.0).astype(bf16)
    rw_v = rw[...]
    rw_col = [jnp.sum(jnp.where(eye, rw_v[j : j + 1, :], 0.0), -1, keepdims=True) for j in range(2)]
    lane_ids = lax.broadcasted_iota(jnp.int32, (S, NS), 1).astype(f32)
    wsel = jnp.where(lane_ids == slot_col[0], rw_col[0], 0.0) + jnp.where(lane_ids == slot_col[1], rw_col[1], 0.0)
    w_hi = wsel.astype(bf16)
    w_lo = (wsel - w_hi.astype(f32)).astype(bf16)

    def project(i, _):
        g = ep_src(i)
        remote(xn.at[g], ga.at[g], s1.at[i], r1.at[i], (g, t)).wait_recv()
        pt[g] = jnp.dot(ga[g], wqkvo[...], preferred_element_type=f32).astype(bf16)
        remote(pt.at[g], qa.at[i], s2.at[i], r2.at[i], (g, t)).start()
        return 0

    lax.fori_loop(1, E, project, 0)

    ld_sn.wait()
    ld_st.wait()

    def arrived(i, _):
        g = ep_peer(i)
        remote(pt.at[g], qa.at[i], s2.at[i], r2.at[i], (g, t)).wait_recv()
        return 0

    lax.fori_loop(1, E, arrived, 0)
    roles = []
    for k in range(4):
        total = qa[0, :, k * 128 : (k + 1) * 128].astype(f32)
        for i in range(1, E):
            total = total + qa[i, :, k * 128 : (k + 1) * 128].astype(f32)
        roles.append(total.astype(bf16).astype(f32))

    for h in range(HN):
        hs = slice(h * HD, (h + 1) * HD)
        qh, kh, vh = roles[0][:, hs], roles[1][:, hs] * HD ** (-0.5), roles[2][:, hs]
        kvq[h, 0] = qh
        kvq[h, 1] = kh
        kvq[h, 2] = vh * iws[h]
        kvq[h, 3] = jnp.broadcast_to(fws[h], (S, HD))
    SB = 8

    def cell(b, _):
        at = pl.ds(pl.multiple_of(b * SB, SB), SB)
        for h in range(HN):
            new = (
                kvq[h, 3, at, :][:, None, :] * state[at, h]
                + kvq[h, 2, at, :][:, :, None] * kvq[h, 1, at, :][:, None, :]
            )
            state[at, h] = new
            nums[h, at, :] = jnp.sum(new * kvq[h, 0, at, :][:, None, :], -1)
        return 0

    lax.fori_loop(0, S // SB, cell, 0)
    out_mat = pltpu.make_async_copy(state, newmat_o, osem.at[0])
    out_mat.start()
    for h in range(HN):
        hs = slice(h * HD, (h + 1) * HD)
        nn = fws[h] * snorm[:, h, :] + iws[h] * kvq[h, 1]
        nnew[:, h, :] = nn
        den = jnp.maximum(jnp.abs(jnp.sum(nn * kvq[h, 0], -1, keepdims=True)), 1.0)
        gate = 1.0 / (1.0 + jnp.exp(-roles[3][:, hs]))
        gated[:, hs] = (gate * nums[h] / den).astype(bf16)
    out_norm = pltpu.make_async_copy(nnew, newnorm_o, osem.at[1])
    out_norm.start()
    out_max = pltpu.make_async_copy(mnew, newmax_o, osem.at[2])
    out_max.start()

    ld_mix.wait()
    gv = gated[...]
    zorder = far_first(Z) + [0]
    for i in zorder:
        zz = zp(i)
        mixs[zz] = jnp.dot(gv, wmix[:, col(zz, o)], preferred_element_type=f32).astype(bf16)
        remote(mixs.at[zz], mixr.at[zz], s3.at[i], r3.at[i], sib).start()
    own = None
    for i in zorder:
        zz = zp(i)
        mine = jnp.dot(gv, wmix[:, col(zz, c)], preferred_element_type=f32)
        remote(mixs.at[zz], mixr.at[zz], s3.at[i], r3.at[i], sib).wait_recv()
        both = mine + mixr[zz].astype(f32)
        if i:
            mixo[zz] = both.astype(bf16)
            remote(mixo.at[zz], rz.at[i], s4.at[i], r4.at[i], z_dev(zz)).start()
        else:
            own = both
    own = own + hid[:, pl.ds(pl.multiple_of(t * W, W), W)].astype(f32)
    for i in near_first(Z):
        remote(mixo.at[zs(i)], rz.at[i], s4.at[i], r4.at[i], z_dev(zs(i))).wait_recv()
        own = own + rz[i].astype(f32)
    so[...] = own.astype(bf16)

    for i in far_first(Z):
        remote(so, st.at[c, z], s5.at[i], r5.at[i], z_dev(zp(i))).start()
    remote(so, st.at[c, z], s6.at[0], r6.at[0], sib).start()
    st[c, z] = so[...]
    disp[:, half(z)] = jnp.dot(chooser, so[...], preferred_element_type=f32).astype(bf16)
    for i in near_first(Z):
        g = zs(i)
        remote(so, st.at[c, g], s5.at[i], r5.at[i], z_dev(g)).wait_recv()
        remote(st.at[c, g], st.at[c, g], s6.at[i], r6.at[i], sib).start()
        disp[:, half(g)] = jnp.dot(chooser, st[c, g], preferred_element_type=f32).astype(bf16)

    def send_rows(i, _):
        p = ep_peer(i)
        remote(disp.at[rows(p)], dx.at[c, rows(e)], s7.at[i], r7.at[i], (p, t)).start()
        return 0

    lax.fori_loop(1, E, send_rows, 0)
    remote(disp.at[rows(e)], dx.at[c, rows(e)], s8.at[0], r8.at[0], sib).start()
    keep = pltpu.make_async_copy(disp.at[rows(e)], dx.at[c, rows(e)], osem.at[3])
    keep.start()

    ld_fg.wait()
    ld_sg.wait()
    ld_su.wait()
    ld_sd.wait()
    for i in range(Z):
        remote(st.at[c, z], st.at[o, zs(i)], s6.at[i], r6.at[i], sib).wait_recv()
    sq = jnp.zeros((S, W), f32)
    for cc in range(2):
        for zz in range(Z):
            v = st[cc, zz].astype(f32)
            sq = sq + v * v
    sscale = lax.rsqrt(jnp.sum(sq, -1, keepdims=True) * (1.0 / D) + NORM_EPS)
    pre = jnp.zeros((S, sgu.shape[0]), f32)
    for cc in range(2):
        for zz in range(Z):
            cs = slice((zz * 2 + cc) * W, (zz * 2 + cc + 1) * W)
            v = (st[cc, zz].astype(f32) * sscale * fgain[:, cs]).astype(bf16)
            pre = pre + lax.dot_general(v, sgu[:, cs], (((1,), (1,)), ((), ())), preferred_element_type=f32)
    SW = sg_h.shape[0]
    sgate, sup = pre[:, :SW], pre[:, SW:]
    shid = (sgate / (1.0 + jnp.exp(-sgate)) * sup).astype(bf16)
    for zz in range(Z):
        shs[zz] = jnp.dot(shid, sdown[:, col(zz, o)], preferred_element_type=f32).astype(bf16)
    remote(shs, shr, s9.at[0], r9.at[0], sib).start()
    for zz in range(Z):
        sho[zz] = jnp.dot(shid, sdown[:, col(zz, c)], preferred_element_type=f32)

    def pass_on(i, _):
        g = ep_src(i)
        remote(disp.at[rows(g)], dx.at[c, rows(g)], s7.at[i], r7.at[i], (g, t)).wait_recv()
        remote(dx.at[c, rows(g)], dx.at[c, rows(g)], s8.at[i], r8.at[i], sib).start()
        return 0

    lax.fori_loop(1, E, pass_on, 0)
    keep.wait()
    wait_bytes(wcat, cat_sem)

    def prepare(cc, sq):
        def piece(zz, sq):
            v = dx[cc, :, half(zz)].astype(f32)
            xg[cc, :, half(zz)] = (v * fgain[:, col(zz, cc)]).astype(bf16)
            v = v * v
            for k in range(W // 128):
                sq = sq + v[:, k * 128 : (k + 1) * 128]
            return sq

        return lax.fori_loop(0, Z, piece, sq)

    sq = prepare(c, jnp.zeros((NS, 128), f32))
    acc[...] = jnp.dot(xg[c], wcat[c], preferred_element_type=f32)

    def from_sibling(i, _):
        g = ep_src(i)
        remote(dx.at[c, rows(g)], dx.at[o, rows(g)], s8.at[i], r8.at[i], sib).wait_recv()
        return 0

    lax.fori_loop(0, E, from_sibling, 0)
    sq = prepare(o, sq)
    acc[...] += jnp.dot(xg[o], wcat[o], preferred_element_type=f32)
    escale = lax.rsqrt(jnp.sum(sq, -1, keepdims=True) * (1.0 / D) + NORM_EPS)
    expert_of = lax.rem(lax.div(lax.broadcasted_iota(jnp.int32, (NS, 128), 0), ROOM), L)
    hids = []
    for j in range(L):
        gv = acc[:, 2 * j * 128 : (2 * j + 1) * 128] * escale
        uv = acc[:, (2 * j + 1) * 128 : (2 * j + 2) * 128] * escale
        hids.append(jnp.where(expert_of == j, gv / (1.0 + jnp.exp(-gv)) * uv, 0.0).astype(bf16))
    hcat = jnp.concatenate(hids, 1)

    ld_ed.wait()

    def down_of(zz, cc):
        total = None
        for j in range(1):
            w = down[:, :, col(zz, cc)].reshape(L * 128, W)
            total = jnp.dot(hcat, w, preferred_element_type=f32)
        return total

    for zz in range(Z):
        po[zz] = down_of(zz, o).astype(bf16)
        remote(po.at[zz], pi.at[zz], s10.at[zz], r10.at[zz], sib).start()
    for zz in range(Z):
        mine = down_of(zz, c)
        remote(po.at[zz], pi.at[zz], s10.at[zz], r10.at[zz], sib).wait_recv()
        ret[:, zz * W : (zz + 1) * W] = (mine + pi[zz].astype(f32)).astype(bf16)

    def send_back(i, _):
        p = ep_peer(i)
        remote(ret.at[rows(p)], rt.at[rows(e)], s11.at[i], r11.at[i], (p, t)).start()
        return 0

    lax.fori_loop(1, E, send_back, 0)
    keep2 = pltpu.make_async_copy(ret.at[rows(e)], rt.at[rows(e)], osem.at[4])
    keep2.start()
    remote(shs, shr, s9.at[0], r9.at[0], sib).wait_recv()
    w_both = jnp.concatenate([w_hi, w_lo], 0)
    keep2.wait()

    def came_back(i, _):
        g = ep_src(i)
        remote(ret.at[rows(g)], rt.at[rows(g)], s11.at[i], r11.at[i], (g, t)).wait_recv()
        return 0

    lax.fori_loop(1, E, came_back, 0)
    own = None
    for i in zorder:
        zz = zp(i)
        two = jnp.dot(w_both, rt[:, half(zz)], preferred_element_type=f32)
        both = two[:S] + two[S:] + sho[zz] + shr[zz].astype(f32)
        if i:
            fin[zz] = both.astype(bf16)
            remote(fin.at[zz], fz.at[i], s12.at[i], r12.at[i], z_dev(zz)).start()
        else:
            own = both
    own = own + so[...].astype(f32)
    for i in near_first(Z):
        remote(fin.at[zs(i)], fz.at[i], s12.at[i], r12.at[i], z_dev(zs(i))).wait_recv()
        own = own + fz[i].astype(f32)
    result_o[...] = own.astype(bf16)

    def drain(i, _):
        p = ep_peer(i)
        remote(xn.at[p], ga.at[e], s1.at[i], r1.at[i], (p, t)).wait_send()
        remote(pt.at[p], qa.at[i], s2.at[i], r2.at[i], (p, t)).wait_send()
        remote(disp.at[rows(p)], dx.at[c, rows(e)], s7.at[i], r7.at[i], (p, t)).wait_send()
        remote(ret.at[rows(p)], rt.at[rows(e)], s11.at[i], r11.at[i], (p, t)).wait_send()
        return 0

    lax.fori_loop(1, E, drain, 0)

    def drain_sib(i, _):
        remote(disp.at[rows(e)], dx.at[c, rows(e)], s8.at[i], r8.at[i], sib).wait_send()
        return 0

    lax.fori_loop(0, E, drain_sib, 0)
    for i in range(Z):
        remote(mixs.at[z], mixr.at[z], s3.at[i], r3.at[i], sib).wait_send()
        remote(so, st.at[c, z], s6.at[i], r6.at[i], sib).wait_send()
        remote(po.at[i], pi.at[i], s10.at[i], r10.at[i], sib).wait_send()
        if i:
            remote(mixo.at[z], rz.at[i], s4.at[i], r4.at[i], z_dev(zp(i))).wait_send()
            remote(so, st.at[c, z], s5.at[i], r5.at[i], z_dev(zp(i))).wait_send()
            remote(fin.at[z], fz.at[i], s12.at[i], r12.at[i], z_dev(zp(i))).wait_send()
    remote(shs, shr, s9.at[0], r9.at[0], sib).wait_send()
    out_mat.wait()
    out_norm.wait()
    out_max.wait()


def per_device(shape, *args):
    (hidden, mgain, wq, wk, wv, wo, wgates, bias, state, snorm, smax, wmix, fgain, routes, rw, eg, eu, ed, sg, su, sd) = args
    E, T = shape["ep"], shape["tp"]
    EX = 4 if E % 4 == 0 and E > 4 else 2
    EY, Z = E // EX, T // 2
    S, D = hidden.shape
    HN, HD = state.shape[1], state.shape[2]
    L, SW = eg.shape[0], sg.shape[1]
    W, KS, NS = D // T, D // E, E * L * ROOM
    f32, bf16 = jnp.float32, jnp.bfloat16
    V, dma = pltpu.VMEM, pltpu.SemaphoreType.DMA
    scratch = [
        V((S, D), bf16), V((1, D), f32), V((KS, 512), bf16), V((2, HN, D), bf16), V(state.shape, f32), V(snorm.shape, f32),
        V((HN, S), f32), V(wmix.shape, bf16), V((1, D), f32), V((2, routes.shape[0]), jnp.int32), V((2, S), f32),
        V((2, D // 2, 4 * 128), bf16), V(ed.shape, bf16), V((2 * SW, D), bf16), V((SW, D), bf16),
        V((E, S, KS), bf16), V((E, S, KS), bf16), V((E, S, 512), bf16), V((E, S, 512), bf16),
        V((HN, 4, S, HD), f32), V((HN, S, HD), f32), V((S, HN * HD), bf16),
        V((Z, S, W), bf16), V((Z, S, W), bf16), V((Z, S, W), bf16), V((Z, S, W), bf16),
        V((S, W), bf16), V((2, Z, S, W), bf16), V((NS, D // 2), bf16), V((2, NS, D // 2), bf16), V((2, NS, D // 2), bf16),
        V((NS, 512), f32), V((Z, NS, W), bf16), V((Z, NS, W), bf16), V((NS, D // 2), bf16), V((NS, D // 2), bf16),
        V((Z, S, W), bf16), V((Z, S, W), bf16), V((Z, S, W), f32), V((Z, S, W), bf16), V((Z, S, W), bf16),
        V(snorm.shape, f32), V((HN, S), f32),
        dma((24,)),
        dma((E,)), dma((E,)), dma((E,)), dma((E,)), dma((Z,)), dma((Z,)), dma((Z,)), dma((Z,)), dma((Z,)), dma((Z,)),
        dma((Z,)), dma((Z,)), dma((E,)), dma((E,)), dma((E,)), dma((E,)), dma((1,)), dma((1,)), dma((Z,)), dma((Z,)),
        dma((E,)), dma((E,)), dma((Z,)), dma((Z,)), dma((5,)),
    ]
    anywhere = pl.BlockSpec(memory_space=pl.ANY)
    hbm = pl.BlockSpec(memory_space=pltpu.HBM)
    in_specs = [hbm] * 21
    in_specs[7] = pl.BlockSpec(memory_space=pltpu.SMEM)
    vm = pl.BlockSpec(memory_space=pltpu.VMEM)
    result, newmat, newnorm, newmax = pl.pallas_call(
        functools.partial(layer_kernel, (EY, EX, Z, S, D, HD, L)),
        out_shape=(
            jax.ShapeDtypeStruct((S, W), bf16),
            jax.ShapeDtypeStruct(state.shape, f32),
            jax.ShapeDtypeStruct(snorm.shape, f32),
            jax.ShapeDtypeStruct((HN, S), f32),
        ),
        in_specs=in_specs,
        out_specs=(vm, anywhere, anywhere, anywhere),
        scratch_shapes=scratch,
        compiler_params=pltpu.CompilerParams(
            collective_id=0, has_side_effects=True, vmem_limit_bytes=48 * 1024 * 1024
        ),
        name="layer",
    )(
        hidden, mgain.reshape(1, D), wq, wk, wv, wo, jnp.swapaxes(wgates, 1, 2), bias, state, snorm, smax.T, wmix,
        fgain.reshape(1, D), routes.T, rw.T, eg, eu, ed, sg.T, su.T, sd,
    )
    return result, newmat, newnorm, newmax.T


def solution(mesh):
    placed = (
        P("ep", None),
        P(),
        P("ep", "tp"),
        P("ep", "tp"),
        P("ep", "tp"),
        P("ep", "tp"),
        P(None, None, "tp"),
        P(None, "tp"),
        P("ep", "tp", None, None),
        P("ep", "tp", None),
        P("ep", "tp"),
        P("tp", None),
        P(),
        P(),
        P("ep", None),
        P("ep", None, "tp"),
        P("ep", None, "tp"),
        P("ep", "tp", None),
        P(None, "tp"),
        P(None, "tp"),
        P("tp", None),
    )
    return jax.shard_map(
        functools.partial(per_device, dict(mesh.shape)),
        mesh=mesh,
        in_specs=placed,
        out_specs=(P("ep", "tp"), P("ep", "tp", None, None), P("ep", "tp", None), P("ep", "tp")),
        check_vma=False,
    )
```

```python
import functools

import jax
import jax.numpy as jnp
from jax import lax
from jax.experimental import pallas as pl
from jax.experimental.pallas import tpu as pltpu
from jax.sharding import PartitionSpec as P

MESH = pl.DeviceIdType.MESH
NORM_EPS = 1e-06
ROOM = 4


def remote(src, dst, send_sem, recv_sem, dev):
    return pltpu.make_async_remote_copy(
        src_ref=src, dst_ref=dst, send_sem=send_sem, recv_sem=recv_sem, device_id=dev, device_id_type=MESH
    )


def wait_bytes(ref, sem):
    pltpu.make_async_copy(ref, ref, sem).wait()


def far_first(n):
    return sorted(range(1, n), key=lambda i: (-min(i, n - i), i))


def near_first(n):
    return sorted(range(1, n), key=lambda i: (min(i, n - i), i))


def layer_kernel(
    cfg,
    hidden_h, mgain_h, wq_h, wk_h, wv_h, wo_h, wg_h, bias_h, state_h, snorm_h, smax_h, wmix_h, fgain_h,
    routes_h, rw_h, eg_h, eu_h, ed_h, sg_h, su_h, sd_h,
    result_o, newmat_o, newnorm_o, newmax_o,
    hid, mgain, wqkvo, wg, bias, state, snorm, smax, wmix, fgain, routes, rw, wcat, down, sgu, sdown,
    xn, ga, pt, qa, kvq, nums, gated, mixs, mixr, mixo, rz, so, st, disp, dx, xg, acc, po, pi, ret, rt, shs, shr, sho, fin, fz,
    nnew, mnew, lsem, s1, r1, s2, r2, s3, r3, s4, r4, s5, r5, s6, r6, s7, r7, s8, r8, s9, r9, s10, r10, s11, r11, s12, r12, osem,
):
    EY, EX, Z, S, D, HD, L = cfg
    E, T = EY * EX, 2 * Z
    W = D // T
    f32, bf16 = jnp.float32, jnp.bfloat16
    e, t = lax.axis_index("ep"), lax.axis_index("tp")
    z, c = lax.div(t, 2), lax.rem(t, 2)
    o = 1 - c
    sib = (e, z * 2 + o)
    y, x = lax.div(e, EX), lax.rem(e, EX)

    def ep_peer(i):
        return lax.rem(y + lax.div(i, EX), EY) * EX + lax.rem(x + lax.rem(i, EX), EX)

    def ep_src(i):
        return lax.rem(y + EY - lax.div(i, EX), EY) * EX + lax.rem(x + EX - lax.rem(i, EX), EX)

    def z_dev(zz):
        return (e, zz * 2 + c)

    def zp(i):
        return lax.rem(z + i, Z)

    def zs(i):
        return lax.rem(z + Z - i, Z)

    def col(zz, cc):
        return pl.ds(pl.multiple_of((zz * 2 + cc) * W, W), W)

    def half(zz):
        return pl.ds(pl.multiple_of(zz * W, W), W)

    def rows(g):
        return pl.ds(pl.multiple_of(g * L * ROOM, L * ROOM), L * ROOM)

    loads = []

    def load(src, dst):
        cp = pltpu.make_async_copy(src, dst, lsem.at[len(loads)])
        cp.start()
        loads.append(cp)
        return cp

    ld_hid = load(hidden_h, hid)
    ld_mg = load(mgain_h, mgain)
    ld_w = [load(w, wqkvo.at[:, k * 128 : (k + 1) * 128]) for k, w in enumerate((wq_h, wk_h, wv_h, wo_h))]
    ld_wg = load(wg_h, wg)
    ld_bi = load(bias_h, bias)
    ld_sm = load(smax_h, smax)
    ld_rt = load(routes_h, routes)
    ld_rw = load(rw_h, rw)
    ld_sn = load(snorm_h, snorm)
    ld_st = load(state_h, state)
    ld_mix = load(wmix_h, wmix)
    ld_fg = load(fgain_h, fgain)
    ld_sg = load(sg_h, sgu.at[0 : sg_h.shape[0], :])
    ld_su = load(su_h, sgu.at[sg_h.shape[0] :, :])
    ld_sd = load(sd_h, sdown)
    ld_ed = load(ed_h, down)
    cat_sem = lsem.at[len(loads)]

    def cat_copies(k):
        zz, cc = lax.div(k, 2), lax.rem(k, 2)
        return [
            pltpu.make_async_copy(
                src.at[j, pl.ds(pl.multiple_of(k * W, W), W), :],
                wcat.at[cc, pl.ds(pl.multiple_of(zz * W, W), W), (2 * j + q) * 128 : (2 * j + q + 1) * 128],
                cat_sem,
            )
            for j in range(L)
            for q, src in enumerate((eg_h, eu_h))
        ]

    def start_cat(k, _):
        for cp in cat_copies(k):
            cp.start()
        return 0

    lax.fori_loop(0, T, start_cat, 0)

    barrier = pltpu.get_barrier_semaphore()

    def greet(i, _):
        pl.semaphore_signal(barrier, inc=1, device_id=(ep_peer(i), t), device_id_type=MESH)
        return 0

    lax.fori_loop(1, E, greet, 0)
    for i in range(1, Z):
        pl.semaphore_signal(barrier, inc=1, device_id=z_dev(zp(i)), device_id_type=MESH)
    pl.semaphore_signal(barrier, inc=1, device_id=sib, device_id_type=MESH)

    ld_hid.wait()
    ld_mg.wait()
    KS = D // E
    sq = jnp.zeros((S, 128), f32)
    for k in range(D // 128):
        v = hid[:, k * 128 : (k + 1) * 128].astype(f32)
        sq = sq + v * v
    scale = lax.rsqrt(jnp.sum(sq, -1, keepdims=True) * (1.0 / D) + NORM_EPS)
    for k in range(E):
        v = hid[:, k * KS : (k + 1) * KS].astype(f32)
        xn[k] = (v * scale * mgain[:, k * KS : (k + 1) * KS]).astype(bf16)

    pl.semaphore_wait(barrier, E - 1 + Z - 1 + 1)

    def send_x(i, _):
        p = ep_peer(i)
        remote(xn.at[p], ga.at[e], s1.at[i], r1.at[i], (p, t)).start()
        return 0

    lax.fori_loop(1, E, send_x, 0)

    for cp in ld_w:
        cp.wait()
    qa[0] = jnp.dot(xn[e], wqkvo[...], preferred_element_type=f32).astype(bf16)

    ld_wg.wait()
    ld_bi.wait()
    ld_sm.wait()
    ld_rt.wait()
    ld_rw.wait()
    HN = 2
    gsum = [[jnp.zeros((S, 128), f32) for _ in range(HN)] for _ in range(2)]
    for k in range(D // 128):
        v = xn[k * 128 // KS, :, (k * 128) % KS : (k * 128) % KS + 128].astype(f32)
        for g in range(2):
            w2 = wg[g, :, k * 128 : (k + 1) * 128].astype(f32)
            for h in range(HN):
                gsum[g][h] = gsum[g][h] + v * w2[h : h + 1, :]
    eye = lax.broadcasted_iota(jnp.int32, (S, S), 0) == lax.broadcasted_iota(jnp.int32, (S, S), 1)
    smax_v = smax[...]
    fws, iws = [], []
    for h in range(HN):
        gi = jnp.sum(gsum[0][h], -1, keepdims=True) + bias[0:1, h : h + 1]
        gf = jnp.sum(gsum[1][h], -1, keepdims=True) + bias[1:2, h : h + 1]
        old = jnp.sum(jnp.where(eye, smax_v[h : h + 1, :], 0.0), -1, keepdims=True)
        carried = jnp.minimum(gf, 0.0) - jnp.log(1.0 + jnp.exp(-jnp.abs(gf))) + old
        nm = jnp.maximum(carried, gi)
        fws.append(jnp.exp(carried - nm))
        iws.append(jnp.exp(gi - nm))
        mnew[h : h + 1, :] = jnp.sum(jnp.where(eye, nm, 0.0), 0, keepdims=True)

    GR = routes_h.shape[1]
    sel = (
        lax.broadcasted_iota(jnp.int32, (S, GR), 1) == lax.broadcasted_iota(jnp.int32, (S, GR), 0) + e * S
    )
    all_routes = routes[...].astype(f32)
    sel_f = jnp.where(sel, 1.0, 0.0)
    r_col = [jnp.sum(sel_f * all_routes[j : j + 1, :], -1, keepdims=True) for j in range(2)]
    r_row = [jnp.sum(jnp.where(eye, r_col[j], 0.0), 0, keepdims=True) for j in range(2)]
    i0 = lax.broadcasted_iota(jnp.int32, (S, S), 0)
    i1 = lax.broadcasted_iota(jnp.int32, (S, S), 1)
    NS = E * L * ROOM
    slot_row, slot_col = [], []
    for j in range(2):
        same = jnp.where(r_col[0] == r_row[j], 1.0, 0.0) + jnp.where(r_col[1] == r_row[j], 1.0, 0.0)
        rank_row = jnp.sum(jnp.where(i0 < i1, same, 0.0), 0, keepdims=True)
        slot_row.append(r_row[j] * ROOM + rank_row)
        same = jnp.where(r_row[0] == r_col[j], 1.0, 0.0) + jnp.where(r_row[1] == r_col[j], 1.0, 0.0)
        rank_col = jnp.sum(jnp.where(i1 < i0, same, 0.0), -1, keepdims=True)
        slot_col.append(r_col[j] * ROOM + rank_col)
    slot_ids = lax.broadcasted_iota(jnp.int32, (NS, S), 0).astype(f32)
    chooser = jnp.where((slot_ids == slot_row[0]) | (slot_ids == slot_row[1]), 1.0, 0.0).astype(bf16)
    rw_v = rw[...]
    rw_col = [jnp.sum(jnp.where(eye, rw_v[j : j + 1, :], 0.0), -1, keepdims=True) for j in range(2)]
    lane_ids = lax.broadcasted_iota(jnp.int32, (S, NS), 1).astype(f32)
    wsel = jnp.where(lane_ids == slot_col[0], rw_col[0], 0.0) + jnp.where(lane_ids == slot_col[1], rw_col[1], 0.0)
    w_hi = wsel.astype(bf16)
    w_lo = (wsel - w_hi.astype(f32)).astype(bf16)

    def project(i, _):
        g = ep_src(i)
        remote(xn.at[g], ga.at[g], s1.at[i], r1.at[i], (g, t)).wait_recv()
        pt[g] = jnp.dot(ga[g], wqkvo[...], preferred_element_type=f32).astype(bf16)
        remote(pt.at[g], qa.at[i], s2.at[i], r2.at[i], (g, t)).start()
        return 0

    lax.fori_loop(1, E, project, 0)

    ld_sn.wait()
    ld_st.wait()

    def arrived(i, _):
        g = ep_peer(i)
        remote(pt.at[g], qa.at[i], s2.at[i], r2.at[i], (g, t)).wait_recv()
        return 0

    lax.fori_loop(1, E, arrived, 0)
    roles = []
    for k in range(4):
        total = qa[0, :, k * 128 : (k + 1) * 128].astype(f32)
        for i in range(1, E):
            total = total + qa[i, :, k * 128 : (k + 1) * 128].astype(f32)
        roles.append(total.astype(bf16).astype(f32))

    for h in range(HN):
        hs = slice(h * HD, (h + 1) * HD)
        qh, kh, vh = roles[0][:, hs], roles[1][:, hs] * HD ** (-0.5), roles[2][:, hs]
        kvq[h, 0] = qh
        kvq[h, 1] = kh
        kvq[h, 2] = vh * iws[h]
        kvq[h, 3] = jnp.broadcast_to(fws[h], (S, HD))
    SB = 8

    def cell(b, _):
        at = pl.ds(pl.multiple_of(b * SB, SB), SB)
        for h in range(HN):
            new = (
                kvq[h, 3, at, :][:, None, :] * state[at, h]
                + kvq[h, 2, at, :][:, :, None] * kvq[h, 1, at, :][:, None, :]
            )
            state[at, h] = new
            nums[h, at, :] = jnp.sum(new * kvq[h, 0, at, :][:, None, :], -1)
        return 0

    lax.fori_loop(0, S // SB, cell, 0)
    out_mat = pltpu.make_async_copy(state, newmat_o, osem.at[0])
    out_mat.start()
    for h in range(HN):
        hs = slice(h * HD, (h + 1) * HD)
        nn = fws[h] * snorm[:, h, :] + iws[h] * kvq[h, 1]
        nnew[:, h, :] = nn
        den = jnp.maximum(jnp.abs(jnp.sum(nn * kvq[h, 0], -1, keepdims=True)), 1.0)
        gate = 1.0 / (1.0 + jnp.exp(-roles[3][:, hs]))
        gated[:, hs] = (gate * nums[h] / den).astype(bf16)
    out_norm = pltpu.make_async_copy(nnew, newnorm_o, osem.at[1])
    out_norm.start()
    out_max = pltpu.make_async_copy(mnew, newmax_o, osem.at[2])
    out_max.start()

    ld_mix.wait()
    gv = gated[...]
    zorder = far_first(Z) + [0]
    for i in zorder:
        zz = zp(i)
        mixs[zz] = jnp.dot(gv, wmix[:, col(zz, o)], preferred_element_type=f32).astype(bf16)
        remote(mixs.at[zz], mixr.at[zz], s3.at[i], r3.at[i], sib).start()
    own = None
    for i in zorder:
        zz = zp(i)
        mine = jnp.dot(gv, wmix[:, col(zz, c)], preferred_element_type=f32)
        remote(mixs.at[zz], mixr.at[zz], s3.at[i], r3.at[i], sib).wait_recv()
        both = mine + mixr[zz].astype(f32)
        if i:
            mixo[zz] = both.astype(bf16)
            remote(mixo.at[zz], rz.at[i], s4.at[i], r4.at[i], z_dev(zz)).start()
        else:
            own = both
    own = own + hid[:, pl.ds(pl.multiple_of(t * W, W), W)].astype(f32)
    for i in near_first(Z):
        remote(mixo.at[zs(i)], rz.at[i], s4.at[i], r4.at[i], z_dev(zs(i))).wait_recv()
        own = own + rz[i].astype(f32)
    so[...] = own.astype(bf16)

    for i in far_first(Z):
        remote(so, st.at[c, z], s5.at[i], r5.at[i], z_dev(zp(i))).start()
    remote(so, st.at[c, z], s6.at[0], r6.at[0], sib).start()
    st[c, z] = so[...]
    disp[:, half(z)] = jnp.dot(chooser, so[...], preferred_element_type=f32).astype(bf16)
    for i in near_first(Z):
        g = zs(i)
        remote(so, st.at[c, g], s5.at[i], r5.at[i], z_dev(g)).wait_recv()
        remote(st.at[c, g], st.at[c, g], s6.at[i], r6.at[i], sib).start()
        disp[:, half(g)] = jnp.dot(chooser, st[c, g], preferred_element_type=f32).astype(bf16)

    def send_rows(i, _):
        p = ep_peer(i)
        remote(disp.at[rows(p)], dx.at[c, rows(e)], s7.at[i], r7.at[i], (p, t)).start()
        return 0

    lax.fori_loop(1, E, send_rows, 0)
    remote(disp.at[rows(e)], dx.at[c, rows(e)], s8.at[0], r8.at[0], sib).start()
    keep = pltpu.make_async_copy(disp.at[rows(e)], dx.at[c, rows(e)], osem.at[3])
    keep.start()

    ld_fg.wait()
    ld_sg.wait()
    ld_su.wait()
    ld_sd.wait()
    for i in range(Z):
        remote(st.at[c, z], st.at[o, zs(i)], s6.at[i], r6.at[i], sib).wait_recv()
    sq = jnp.zeros((S, W), f32)
    for cc in range(2):
        for zz in range(Z):
            v = st[cc, zz].astype(f32)
            sq = sq + v * v
    sscale = lax.rsqrt(jnp.sum(sq, -1, keepdims=True) * (1.0 / D) + NORM_EPS)
    pre = jnp.zeros((S, sgu.shape[0]), f32)
    for cc in range(2):
        for zz in range(Z):
            cs = slice((zz * 2 + cc) * W, (zz * 2 + cc + 1) * W)
            v = (st[cc, zz].astype(f32) * sscale * fgain[:, cs]).astype(bf16)
            pre = pre + lax.dot_general(v, sgu[:, cs], (((1,), (1,)), ((), ())), preferred_element_type=f32)
    SW = sg_h.shape[0]
    sgate, sup = pre[:, :SW], pre[:, SW:]
    shid = (sgate / (1.0 + jnp.exp(-sgate)) * sup).astype(bf16)
    for zz in range(Z):
        shs[zz] = jnp.dot(shid, sdown[:, col(zz, o)], preferred_element_type=f32).astype(bf16)
    remote(shs, shr, s9.at[0], r9.at[0], sib).start()
    for zz in range(Z):
        sho[zz] = jnp.dot(shid, sdown[:, col(zz, c)], preferred_element_type=f32)

    def pass_on(i, _):
        g = ep_src(i)
        remote(disp.at[rows(g)], dx.at[c, rows(g)], s7.at[i], r7.at[i], (g, t)).wait_recv()
        remote(dx.at[c, rows(g)], dx.at[c, rows(g)], s8.at[i], r8.at[i], sib).start()
        return 0

    lax.fori_loop(1, E, pass_on, 0)
    keep.wait()
    wait_bytes(wcat, cat_sem)

    def prepare(cc, sq):
        def piece(zz, sq):
            v = dx[cc, :, half(zz)].astype(f32)
            xg[cc, :, half(zz)] = (v * fgain[:, col(zz, cc)]).astype(bf16)
            v = v * v
            for k in range(W // 128):
                sq = sq + v[:, k * 128 : (k + 1) * 128]
            return sq

        return lax.fori_loop(0, Z, piece, sq)

    sq = prepare(c, jnp.zeros((NS, 128), f32))
    acc[...] = jnp.dot(xg[c], wcat[c], preferred_element_type=f32)

    def from_sibling(i, _):
        g = ep_src(i)
        remote(dx.at[c, rows(g)], dx.at[o, rows(g)], s8.at[i], r8.at[i], sib).wait_recv()
        return 0

    lax.fori_loop(0, E, from_sibling, 0)
    sq = prepare(o, sq)
    acc[...] += jnp.dot(xg[o], wcat[o], preferred_element_type=f32)
    escale = lax.rsqrt(jnp.sum(sq, -1, keepdims=True) * (1.0 / D) + NORM_EPS)
    expert_of = lax.rem(lax.div(lax.broadcasted_iota(jnp.int32, (NS, 128), 0), ROOM), L)
    hids = []
    for j in range(L):
        gv = acc[:, 2 * j * 128 : (2 * j + 1) * 128] * escale
        uv = acc[:, (2 * j + 1) * 128 : (2 * j + 2) * 128] * escale
        hids.append(jnp.where(expert_of == j, gv / (1.0 + jnp.exp(-gv)) * uv, 0.0).astype(bf16))
    hcat = jnp.concatenate(hids, 1)

    ld_ed.wait()

    def down_of(zz, cc):
        total = None
        for j in range(1):
            w = down[:, :, col(zz, cc)].reshape(L * 128, W)
            total = jnp.dot(hcat, w, preferred_element_type=f32)
        return total

    for zz in range(Z):
        po[zz] = down_of(zz, o).astype(bf16)
        remote(po.at[zz], pi.at[zz], s10.at[zz], r10.at[zz], sib).start()
    for zz in range(Z):
        mine = down_of(zz, c)
        remote(po.at[zz], pi.at[zz], s10.at[zz], r10.at[zz], sib).wait_recv()
        ret[:, zz * W : (zz + 1) * W] = (mine + pi[zz].astype(f32)).astype(bf16)

    def send_back(i, _):
        p = ep_peer(i)
        remote(ret.at[rows(p)], rt.at[rows(e)], s11.at[i], r11.at[i], (p, t)).start()
        return 0

    lax.fori_loop(1, E, send_back, 0)
    keep2 = pltpu.make_async_copy(ret.at[rows(e)], rt.at[rows(e)], osem.at[4])
    keep2.start()
    remote(shs, shr, s9.at[0], r9.at[0], sib).wait_recv()
    w_both = jnp.concatenate([w_hi, w_lo], 0)
    keep2.wait()

    def came_back(i, _):
        g = ep_src(i)
        remote(ret.at[rows(g)], rt.at[rows(g)], s11.at[i], r11.at[i], (g, t)).wait_recv()
        return 0

    lax.fori_loop(1, E, came_back, 0)
    own = None
    for i in zorder:
        zz = zp(i)
        two = jnp.dot(w_both, rt[:, half(zz)], preferred_element_type=f32)
        both = two[:S] + two[S:] + sho[zz] + shr[zz].astype(f32)
        if i:
            fin[zz] = both.astype(bf16)
            remote(fin.at[zz], fz.at[i], s12.at[i], r12.at[i], z_dev(zz)).start()
        else:
            own = both
    own = own + so[...].astype(f32)
    for i in near_first(Z):
        remote(fin.at[zs(i)], fz.at[i], s12.at[i], r12.at[i], z_dev(zs(i))).wait_recv()
        own = own + fz[i].astype(f32)
    result_o[...] = own.astype(bf16)

    def drain(i, _):
        p = ep_peer(i)
        remote(xn.at[p], ga.at[e], s1.at[i], r1.at[i], (p, t)).wait_send()
        remote(pt.at[p], qa.at[i], s2.at[i], r2.at[i], (p, t)).wait_send()
        remote(disp.at[rows(p)], dx.at[c, rows(e)], s7.at[i], r7.at[i], (p, t)).wait_send()
        remote(ret.at[rows(p)], rt.at[rows(e)], s11.at[i], r11.at[i], (p, t)).wait_send()
        return 0

    lax.fori_loop(1, E, drain, 0)

    def drain_sib(i, _):
        remote(disp.at[rows(e)], dx.at[c, rows(e)], s8.at[i], r8.at[i], sib).wait_send()
        return 0

    lax.fori_loop(0, E, drain_sib, 0)
    for i in range(Z):
        remote(mixs.at[z], mixr.at[z], s3.at[i], r3.at[i], sib).wait_send()
        remote(so, st.at[c, z], s6.at[i], r6.at[i], sib).wait_send()
        remote(po.at[i], pi.at[i], s10.at[i], r10.at[i], sib).wait_send()
        if i:
            remote(mixo.at[z], rz.at[i], s4.at[i], r4.at[i], z_dev(zp(i))).wait_send()
            remote(so, st.at[c, z], s5.at[i], r5.at[i], z_dev(zp(i))).wait_send()
            remote(fin.at[z], fz.at[i], s12.at[i], r12.at[i], z_dev(zp(i))).wait_send()
    remote(shs, shr, s9.at[0], r9.at[0], sib).wait_send()
    out_mat.wait()
    out_norm.wait()
    out_max.wait()


def store_kernel(*refs):
    n = len(refs) // 2
    sem = refs[-1]
    copies = [pltpu.make_async_copy(refs[i], refs[n + i], sem.at[i]) for i in range(n)]
    for cp in copies:
        cp.start()
    for cp in copies:
        cp.wait()


def per_device(shape, *args):
    (hidden, mgain, wq, wk, wv, wo, wgates, bias, state, snorm, smax, wmix, fgain, routes, rw, eg, eu, ed, sg, su, sd) = args
    E, T = shape["ep"], shape["tp"]
    EX = 4 if E % 4 == 0 and E > 4 else 2
    EY, Z = E // EX, T // 2
    S, D = hidden.shape
    HN, HD = state.shape[1], state.shape[2]
    L, SW = eg.shape[0], sg.shape[1]
    W, KS, NS = D // T, D // E, E * L * ROOM
    f32, bf16 = jnp.float32, jnp.bfloat16
    V, dma = pltpu.VMEM, pltpu.SemaphoreType.DMA
    scratch = [
        V((S, D), bf16), V((1, D), f32), V((KS, 512), bf16), V((2, HN, D), bf16), V((2, HN), f32), V(state.shape, f32), V(snorm.shape, f32),
        V((HN, S), f32), V(wmix.shape, bf16), V((1, D), f32), V((2, routes.shape[0]), jnp.int32), V((2, S), f32),
        V((2, D // 2, 4 * 128), bf16), V(ed.shape, bf16), V((2 * SW, D), bf16), V((SW, D), bf16),
        V((E, S, KS), bf16), V((E, S, KS), bf16), V((E, S, 512), bf16), V((E, S, 512), bf16),
        V((HN, 4, S, HD), f32), V((HN, S, HD), f32), V((S, HN * HD), bf16),
        V((Z, S, W), bf16), V((Z, S, W), bf16), V((Z, S, W), bf16), V((Z, S, W), bf16),
        V((S, W), bf16), V((2, Z, S, W), bf16), V((NS, D // 2), bf16), V((2, NS, D // 2), bf16), V((2, NS, D // 2), bf16),
        V((NS, 512), f32), V((Z, NS, W), bf16), V((Z, NS, W), bf16), V((NS, D // 2), bf16), V((NS, D // 2), bf16),
        V((Z, S, W), bf16), V((Z, S, W), bf16), V((Z, S, W), f32), V((Z, S, W), bf16), V((Z, S, W), bf16),
        V(snorm.shape, f32), V((HN, S), f32),
        dma((24,)),
        dma((E,)), dma((E,)), dma((E,)), dma((E,)), dma((Z,)), dma((Z,)), dma((Z,)), dma((Z,)), dma((Z,)), dma((Z,)),
        dma((Z,)), dma((Z,)), dma((E,)), dma((E,)), dma((E,)), dma((E,)), dma((1,)), dma((1,)), dma((Z,)), dma((Z,)),
        dma((E,)), dma((E,)), dma((Z,)), dma((Z,)), dma((5,)),
    ]
    anywhere = pl.BlockSpec(memory_space=pl.ANY)
    operands = (
        hidden, mgain.reshape(1, D), wq, wk, wv, wo, jnp.swapaxes(wgates, 1, 2), bias, state, snorm, smax.T, wmix,
        fgain.reshape(1, D), routes.T, rw.T, eg, eu, ed, sg.T, su.T, sd,
    )
    results = ((S, W), bf16), (state.shape, f32), (snorm.shape, f32), ((HN, S), f32)
    inner = pl.pallas_call(
        functools.partial(layer_kernel, (EY, EX, Z, S, D, HD, L)),
        out_shape=tuple(V(*r) for r in results),
        in_specs=[anywhere] * len(operands),
        out_specs=(pl.BlockSpec(memory_space=V), anywhere, anywhere, anywhere),
        scratch_shapes=scratch,
        compiler_params=pltpu.CompilerParams(
            collective_id=0, has_side_effects=True, vmem_limit_bytes=48 * 1024 * 1024
        ),
        name="layer",
    )(*(pltpu.with_memory_space_constraint(a, pltpu.HBM) for a in operands))
    result, newmat, newnorm, newmax = pl.pallas_call(
        store_kernel,
        out_shape=tuple(jax.ShapeDtypeStruct(*r) for r in results),
        in_specs=[anywhere] * len(results),
        out_specs=(anywhere,) * len(results),
        scratch_shapes=[dma((len(results),))],
        compiler_params=pltpu.CompilerParams(vmem_limit_bytes=1024 * 1024),
        name="store",
    )(*(pltpu.with_memory_space_constraint(a, V) for a in inner))
    return result, newmat, newnorm, newmax.T


def solution(mesh):
    placed = (
        P("ep", None),
        P(),
        P("ep", "tp"),
        P("ep", "tp"),
        P("ep", "tp"),
        P("ep", "tp"),
        P(None, None, "tp"),
        P(None, "tp"),
        P("ep", "tp", None, None),
        P("ep", "tp", None),
        P("ep", "tp"),
        P("tp", None),
        P(),
        P(),
        P("ep", None),
        P("ep", None, "tp"),
        P("ep", None, "tp"),
        P("ep", "tp", None),
        P(None, "tp"),
        P(None, "tp"),
        P("tp", None),
    )
    return jax.shard_map(
        functools.partial(per_device, dict(mesh.shape)),
        mesh=mesh,
        in_specs=placed,
        out_specs=(P("ep", "tp"), P("ep", "tp", None, None), P("ep", "tp", None), P("ep", "tp")),
        check_vma=False,
    )
```

```python
import functools

import jax
import jax.numpy as jnp
from jax import lax
from jax.experimental import pallas as pl
from jax.experimental.pallas import tpu as pltpu
from jax.sharding import PartitionSpec as P

MESH = pl.DeviceIdType.MESH
NORM_EPS = 1e-06
ROOM = 4


def remote(src, dst, send_sem, recv_sem, dev):
    return pltpu.make_async_remote_copy(
        src_ref=src, dst_ref=dst, send_sem=send_sem, recv_sem=recv_sem, device_id=dev, device_id_type=MESH
    )


def wait_bytes(ref, sem):
    pltpu.make_async_copy(ref, ref, sem).wait()


def far_first(n):
    return sorted(range(1, n), key=lambda i: (-min(i, n - i), i))


def near_first(n):
    return sorted(range(1, n), key=lambda i: (min(i, n - i), i))


def layer_kernel(
    cfg,
    hidden_h, mgain_h, wq_h, wk_h, wv_h, wo_h, wg_h, bias_h, state_h, snorm_h, smax_h, wmix_h, fgain_h,
    routes_h, rw_h, eg_h, eu_h, ed_h, sg_h, su_h, sd_h,
    result_o, newmat_o, newnorm_o, newmax_o,
    hid, mgain, wqkvo, wg, bias, state, snorm, smax, wmix, fgain, routes, rw, wcat, down, sgu, sdown,
    xn, ga, pt, qa, kvq, nums, gated, mixs, mixr, mixm, mixo, rz, so, st, disp, dx, xg, xs, acc, po, pi, ret, rt,
    shs, shr, sho, fin, fz, nnew, mnew,
    lsem, bulk, sends, r1, r2, r3, r4, r5, r6, r7, r8, r9, r10, r11, r12, osem,
):
    EY, EX, Z, S, D, HD, L = cfg
    E, T = EY * EX, 2 * Z
    W = D // T
    f32, bf16 = jnp.float32, jnp.bfloat16
    e, t = lax.axis_index("ep"), lax.axis_index("tp")
    z, c = lax.div(t, 2), lax.rem(t, 2)
    o = 1 - c
    sib = (e, z * 2 + o)
    y, x = lax.div(e, EX), lax.rem(e, EX)
    s1, s2, s3, s4, s5, s6, s7, s8, s9, s10, s11, s12 = (sends.at[k] for k in range(12))

    def ep_peer(i):
        return lax.rem(y + lax.div(i, EX), EY) * EX + lax.rem(x + lax.rem(i, EX), EX)

    def ep_src(i):
        return lax.rem(y + EY - lax.div(i, EX), EY) * EX + lax.rem(x + EX - lax.rem(i, EX), EX)

    def z_dev(zz):
        return (e, zz * 2 + c)

    def zp(i):
        return lax.rem(z + i, Z)

    def zs(i):
        return lax.rem(z + Z - i, Z)

    def col(zz, cc):
        return pl.ds(pl.multiple_of((zz * 2 + cc) * W, W), W)

    def half(zz):
        return pl.ds(pl.multiple_of(zz * W, W), W)

    def rows(g):
        return pl.ds(pl.multiple_of(g * L * ROOM, L * ROOM), L * ROOM)

    def each(first, n, step):
        def one(i, _):
            step(i)
            return 0

        lax.fori_loop(first, n, one, 0)

    barrier = pltpu.get_barrier_semaphore()

    def greet(dev):
        pl.semaphore_signal(barrier, inc=1, device_id=dev, device_id_type=MESH)

    loads = []

    def load(src, dst):
        cp = pltpu.make_async_copy(src, dst, lsem.at[len(loads)])
        cp.start()
        loads.append(cp)
        return cp

    ld_hid = load(hidden_h, hid)
    ld_mg = load(mgain_h, mgain)
    each(1, E, lambda i: greet((ep_peer(i), t)))
    for i in far_first(Z):
        greet(z_dev(zp(i)))
    greet(sib)
    for k, w in enumerate((wq_h, wk_h, wv_h, wo_h)):
        pltpu.make_async_copy(w, wqkvo.at[:, k * 128 : (k + 1) * 128], bulk.at[0]).start()

    ld_hid.wait()
    ld_mg.wait()
    KS = D // E
    sq = jnp.zeros((S, 128), f32)
    for k in range(D // 128):
        v = hid[:, k * 128 : (k + 1) * 128].astype(f32)
        sq = sq + v * v
    scale = lax.rsqrt(jnp.sum(sq, -1, keepdims=True) * (1.0 / D) + NORM_EPS)
    for k in range(E):
        v = hid[:, k * KS : (k + 1) * KS].astype(f32)
        xn[k] = (v * scale * mgain[:, k * KS : (k + 1) * KS]).astype(bf16)
    pl.semaphore_wait(barrier, E - 1 + Z - 1 + 1)

    def send_x(i):
        p = ep_peer(i)
        remote(xn.at[p], ga.at[e], s1, r1.at[i], (p, t)).start()

    each(1, E, send_x)

    ld_wg = load(wg_h, wg)
    ld_bi = load(bias_h, bias)
    ld_sm = load(smax_h, smax)
    ld_rt = load(routes_h, routes)
    ld_rw = load(rw_h, rw)
    ld_sn = load(snorm_h, snorm)
    ld_st = load(state_h, state)
    ld_fg = load(fgain_h, fgain)
    SW = sg_h.shape[0]

    def start_narrow(k):
        zz, cc = lax.div(k, 2), lax.rem(k, 2)
        cols = pl.ds(pl.multiple_of(k * W, W), W)
        pltpu.make_async_copy(wmix_h.at[:, cols], wmix.at[cc, :, half(zz)], bulk.at[1]).start()
        pltpu.make_async_copy(sg_h.at[:, cols], sgu.at[cc, 0:SW, half(zz)], bulk.at[2]).start()
        pltpu.make_async_copy(su_h.at[:, cols], sgu.at[cc, SW : 2 * SW, half(zz)], bulk.at[2]).start()
        pltpu.make_async_copy(sd_h.at[:, cols], sdown.at[cc, :, half(zz)], bulk.at[3]).start()

    def start_wide(k):
        zz, cc = lax.div(k, 2), lax.rem(k, 2)
        cols = pl.ds(pl.multiple_of(k * W, W), W)
        for j in range(L):
            for q, src in enumerate((eg_h, eu_h)):
                lanes = slice((2 * j + q) * 128, (2 * j + q + 1) * 128)
                pltpu.make_async_copy(src.at[j, cols, :], wcat.at[cc, half(zz), lanes], bulk.at[4]).start()
            pltpu.make_async_copy(
                ed_h.at[j, :, cols], down.at[cc, j * 128 : (j + 1) * 128, half(zz)], bulk.at[5]
            ).start()

    each(0, T, start_narrow)
    each(0, T, start_wide)

    wait_bytes(wqkvo, bulk.at[0])
    qa[0] = jnp.dot(xn[e], wqkvo[...], preferred_element_type=f32).astype(bf16)

    def project(i):
        g = ep_src(i)
        remote(xn.at[g], ga.at[g], s1, r1.at[i], (g, t)).wait_recv()
        pt[g] = jnp.dot(ga[g], wqkvo[...], preferred_element_type=f32).astype(bf16)
        remote(pt.at[g], qa.at[i], s2, r2.at[0], (g, t)).start()

    each(1, E, project)

    ld_wg.wait()
    ld_bi.wait()
    ld_sm.wait()
    ld_rt.wait()
    ld_rw.wait()
    HN = 2
    gsum = [[jnp.zeros((S, 128), f32) for _ in range(HN)] for _ in range(2)]
    for k in range(D // 128):
        v = xn[k * 128 // KS, :, (k * 128) % KS : (k * 128) % KS + 128].astype(f32)
        for g in range(2):
            w2 = wg[g, :, k * 128 : (k + 1) * 128].astype(f32)
            for h in range(HN):
                gsum[g][h] = gsum[g][h] + v * w2[h : h + 1, :]
    eye = lax.broadcasted_iota(jnp.int32, (S, S), 0) == lax.broadcasted_iota(jnp.int32, (S, S), 1)
    smax_v = smax[...]
    fws, iws = [], []
    for h in range(HN):
        gi = jnp.sum(gsum[0][h], -1, keepdims=True) + bias[0:1, h : h + 1]
        gf = jnp.sum(gsum[1][h], -1, keepdims=True) + bias[1:2, h : h + 1]
        old = jnp.sum(jnp.where(eye, smax_v[h : h + 1, :], 0.0), -1, keepdims=True)
        carried = jnp.minimum(gf, 0.0) - jnp.log(1.0 + jnp.exp(-jnp.abs(gf))) + old
        nm = jnp.maximum(carried, gi)
        fws.append(jnp.exp(carried - nm))
        iws.append(jnp.exp(gi - nm))
        mnew[h : h + 1, :] = jnp.sum(jnp.where(eye, nm, 0.0), 0, keepdims=True)
    out_max = pltpu.make_async_copy(mnew, newmax_o, osem.at[2])
    out_max.start()

    GR = routes_h.shape[1]
    sel = (
        lax.broadcasted_iota(jnp.int32, (S, GR), 1) == lax.broadcasted_iota(jnp.int32, (S, GR), 0) + e * S
    )
    all_routes = routes[...].astype(f32)
    sel_f = jnp.where(sel, 1.0, 0.0)
    r_col = [jnp.sum(sel_f * all_routes[j : j + 1, :], -1, keepdims=True) for j in range(2)]
    r_row = [jnp.sum(jnp.where(eye, r_col[j], 0.0), 0, keepdims=True) for j in range(2)]
    i0 = lax.broadcasted_iota(jnp.int32, (S, S), 0)
    i1 = lax.broadcasted_iota(jnp.int32, (S, S), 1)
    NS = E * L * ROOM
    slot_row, slot_col = [], []
    for j in range(2):
        same = jnp.where(r_col[0] == r_row[j], 1.0, 0.0) + jnp.where(r_col[1] == r_row[j], 1.0, 0.0)
        rank_row = jnp.sum(jnp.where(i0 < i1, same, 0.0), 0, keepdims=True)
        slot_row.append(r_row[j] * ROOM + rank_row)
        same = jnp.where(r_row[0] == r_col[j], 1.0, 0.0) + jnp.where(r_row[1] == r_col[j], 1.0, 0.0)
        rank_col = jnp.sum(jnp.where(i1 < i0, same, 0.0), -1, keepdims=True)
        slot_col.append(r_col[j] * ROOM + rank_col)
    slot_ids = lax.broadcasted_iota(jnp.int32, (NS, S), 0).astype(f32)
    chooser = jnp.where((slot_ids == slot_row[0]) | (slot_ids == slot_row[1]), 1.0, 0.0).astype(bf16)
    rw_v = rw[...]
    rw_col = [jnp.sum(jnp.where(eye, rw_v[j : j + 1, :], 0.0), -1, keepdims=True) for j in range(2)]
    lane_ids = lax.broadcasted_iota(jnp.int32, (S, NS), 1).astype(f32)
    wsel = jnp.where(lane_ids == slot_col[0], rw_col[0], 0.0) + jnp.where(lane_ids == slot_col[1], rw_col[1], 0.0)
    w_hi = wsel.astype(bf16)
    w_lo = (wsel - w_hi.astype(f32)).astype(bf16)
    w_both = jnp.concatenate([w_hi, w_lo], 0)

    ld_sn.wait()
    ld_st.wait()
    wait_bytes(qa.at[pl.ds(1, E - 1)], r2.at[0])
    roles = []
    for k in range(4):
        total = qa[0, :, k * 128 : (k + 1) * 128].astype(f32)
        for i in range(1, E):
            total = total + qa[i, :, k * 128 : (k + 1) * 128].astype(f32)
        roles.append(total.astype(bf16).astype(f32))

    for h in range(HN):
        hs = slice(h * HD, (h + 1) * HD)
        qh, kh, vh = roles[0][:, hs], roles[1][:, hs] * HD ** (-0.5), roles[2][:, hs]
        kvq[h, 0] = qh
        kvq[h, 1] = kh
        kvq[h, 2] = vh * iws[h]
        kvq[h, 3] = jnp.broadcast_to(fws[h], (S, HD))
    SB = 8

    def cell(b):
        at = pl.ds(pl.multiple_of(b * SB, SB), SB)
        for h in range(HN):
            new = (
                kvq[h, 3, at, :][:, None, :] * state[at, h]
                + kvq[h, 2, at, :][:, :, None] * kvq[h, 1, at, :][:, None, :]
            )
            state[at, h] = new
            nums[h, at, :] = jnp.sum(new * kvq[h, 0, at, :][:, None, :], -1)

    each(0, S // SB, cell)
    out_mat = pltpu.make_async_copy(state, newmat_o, osem.at[0])
    out_mat.start()
    for h in range(HN):
        hs = slice(h * HD, (h + 1) * HD)
        nn = fws[h] * snorm[:, h, :] + iws[h] * kvq[h, 1]
        nnew[:, h, :] = nn
        den = jnp.maximum(jnp.abs(jnp.sum(nn * kvq[h, 0], -1, keepdims=True)), 1.0)
        gate = 1.0 / (1.0 + jnp.exp(-roles[3][:, hs]))
        gated[:, hs] = (gate * nums[h] / den).astype(bf16)
    out_norm = pltpu.make_async_copy(nnew, newnorm_o, osem.at[1])
    out_norm.start()

    wait_bytes(wmix, bulk.at[1])
    gv = gated[...]
    zorder = far_first(Z) + [0]
    theirs = jnp.dot(gv, wmix[o], preferred_element_type=f32)
    for zz in range(Z):
        mixs[zz] = theirs[:, zz * W : (zz + 1) * W].astype(bf16)
    for i in zorder:
        remote(mixs.at[zp(i)], mixr.at[zp(i)], s3, r3.at[i], sib).start()
    mine = jnp.dot(gv, wmix[c], preferred_element_type=f32)
    for zz in range(Z):
        mixm[zz] = mine[:, zz * W : (zz + 1) * W]
    own = None
    for i in zorder:
        zz = zp(i)
        remote(mixs.at[zz], mixr.at[zz], s3, r3.at[i], sib).wait_recv()
        both = mixm[zz] + mixr[zz].astype(f32)
        if i:
            mixo[i] = both.astype(bf16)
            remote(mixo.at[i], rz.at[i], s4, r4.at[0], z_dev(zz)).start()
        else:
            own = both
    own = own + hid[:, pl.ds(pl.multiple_of(t * W, W), W)].astype(f32)
    wait_bytes(rz.at[pl.ds(1, Z - 1)], r4.at[0])
    for i in range(1, Z):
        own = own + rz[i].astype(f32)
    so[...] = own.astype(bf16)

    for i in far_first(Z):
        remote(so, st.at[c, z], s5, r5.at[i], z_dev(zp(i))).start()

    def dispatch(block, g):
        disp[:, half(g)] = jnp.dot(chooser, block, preferred_element_type=f32).astype(bf16)

        def send_rows(i):
            p = ep_peer(i)
            remote(disp.at[rows(p), half(g)], dx.at[c, rows(e), half(g)], s7, r7.at[i], (p, t)).start()

        each(1, E, send_rows)
        pltpu.make_async_copy(disp.at[rows(e), half(g)], dx.at[c, rows(e), half(g)], r7.at[0]).start()

    dispatch(so[...], z)
    remote(so, st.at[c, z], s6, r6.at[0], sib).start()
    st[c, z] = so[...]
    for i in near_first(Z):
        g = zs(i)
        remote(so, st.at[c, g], s5, r5.at[i], z_dev(g)).wait_recv()
        dispatch(st[c, g], g)
        remote(st.at[c, g], st.at[c, g], s6, r6.at[0], sib).start()

    ld_fg.wait()
    wait_bytes(sgu, bulk.at[2])
    wait_bytes(sdown, bulk.at[3])
    wait_bytes(st.at[o], r6.at[0])
    sq = jnp.zeros((S, W), f32)
    for cc in range(2):
        for zz in range(Z):
            v = st[cc, zz].astype(f32)
            sq = sq + v * v
    sscale = lax.rsqrt(jnp.sum(sq, -1, keepdims=True) * (1.0 / D) + NORM_EPS)
    pre = jnp.zeros((S, 2 * SW), f32)
    for cc in range(2):
        for zz in range(Z):
            cs = slice((zz * 2 + cc) * W, (zz * 2 + cc + 1) * W)
            xs[:, zz * W : (zz + 1) * W] = (st[cc, zz].astype(f32) * sscale * fgain[:, cs]).astype(bf16)
        pre = pre + lax.dot_general(xs[...], sgu[cc], (((1,), (1,)), ((), ())), preferred_element_type=f32)
    sgate, sup = pre[:, :SW], pre[:, SW:]
    shid = (sgate / (1.0 + jnp.exp(-sgate)) * sup).astype(bf16)
    theirs = jnp.dot(shid, sdown[o], preferred_element_type=f32)
    for zz in range(Z):
        shs[zz] = theirs[:, zz * W : (zz + 1) * W].astype(bf16)
    remote(shs, shr, s9, r9.at[0], sib).start()
    mine = jnp.dot(shid, sdown[c], preferred_element_type=f32)
    for zz in range(Z):
        sho[zz] = mine[:, zz * W : (zz + 1) * W]

    def pass_on(i):
        g = ep_src(i)
        wait_bytes(dx.at[c, rows(g)], r7.at[i])
        remote(dx.at[c, rows(g)], dx.at[c, rows(g)], s8, r8.at[0], sib).start()

    each(0, E, pass_on)
    wait_bytes(wcat, bulk.at[4])

    def prepare(cc, sq):
        def piece(zz, sq):
            v = dx[cc, :, half(zz)].astype(f32)
            xg[:, half(zz)] = (v * fgain[:, col(zz, cc)]).astype(bf16)
            v = v * v
            for k in range(W // 128):
                sq = sq + v[:, k * 128 : (k + 1) * 128]
            return sq

        return lax.fori_loop(0, Z, piece, sq)

    sq = prepare(c, jnp.zeros((NS, 128), f32))
    acc[...] = jnp.dot(xg[...], wcat[c], preferred_element_type=f32)
    wait_bytes(dx.at[o], r8.at[0])
    sq = prepare(o, sq)
    acc[...] += jnp.dot(xg[...], wcat[o], preferred_element_type=f32)
    escale = lax.rsqrt(jnp.sum(sq, -1, keepdims=True) * (1.0 / D) + NORM_EPS)
    expert_of = lax.rem(lax.div(lax.broadcasted_iota(jnp.int32, (NS, 128), 0), ROOM), L)
    hids = []
    for j in range(L):
        gv = acc[:, 2 * j * 128 : (2 * j + 1) * 128] * escale
        uv = acc[:, (2 * j + 1) * 128 : (2 * j + 2) * 128] * escale
        hids.append(jnp.where(expert_of == j, gv / (1.0 + jnp.exp(-gv)) * uv, 0.0).astype(bf16))
    hcat = jnp.concatenate(hids, 1)

    wait_bytes(down, bulk.at[5])
    LAG = min(3, Z)

    def down_theirs(i):
        zz = zp(i)
        po[i] = jnp.dot(hcat, down[o, :, half(zz)], preferred_element_type=f32).astype(bf16)
        remote(po.at[i], pi.at[i], s10, r10.at[i], sib).start()

    def down_mine(i):
        zz = zp(i)
        part = jnp.dot(hcat, down[c, :, half(zz)], preferred_element_type=f32)
        remote(po.at[i], pi.at[i], s10, r10.at[i], sib).wait_recv()
        ret[:, half(zz)] = (part + pi[i].astype(f32)).astype(bf16)

        def send_back(k):
            p = ep_peer(k)
            remote(ret.at[rows(p), half(zz)], rt.at[rows(e), half(zz)], s11, r11.at[i], (p, t)).start()

        each(1, E, send_back)
        pltpu.make_async_copy(ret.at[rows(e), half(zz)], rt.at[rows(e), half(zz)], r11.at[i]).start()

    for k in range(Z + LAG):
        if k < Z:
            down_theirs(zorder[k])
        if k >= LAG:
            down_mine(zorder[k - LAG])

    remote(shs, shr, s9, r9.at[0], sib).wait_recv()
    own = None
    for i in zorder:
        zz = zp(i)
        wait_bytes(rt.at[:, half(zz)], r11.at[i])
        two = jnp.dot(w_both, rt[:, half(zz)], preferred_element_type=f32)
        both = two[:S] + two[S:] + sho[zz] + shr[zz].astype(f32)
        if i:
            fin[i] = both.astype(bf16)
            remote(fin.at[i], fz.at[i], s12, r12.at[0], z_dev(zz)).start()
        else:
            own = both
    own = own + so[...].astype(f32)
    wait_bytes(fz.at[pl.ds(1, Z - 1)], r12.at[0])
    for i in range(1, Z):
        own = own + fz[i].astype(f32)
    result_o[...] = own.astype(bf16)

    wait_bytes(xn.at[pl.ds(1, E - 1)], s1)
    wait_bytes(pt.at[pl.ds(1, E - 1)], s2)
    wait_bytes(mixs, s3)
    wait_bytes(mixo.at[pl.ds(1, Z - 1)], s4)
    wait_bytes(mixo.at[pl.ds(1, Z - 1)], s5)
    wait_bytes(mixs, s6)
    wait_bytes(disp.at[pl.ds(0, NS - L * ROOM)], s7)
    wait_bytes(disp, s8)
    wait_bytes(shs, s9)
    wait_bytes(po, s10)
    wait_bytes(ret.at[pl.ds(0, NS - L * ROOM)], s11)
    wait_bytes(fin.at[pl.ds(1, Z - 1)], s12)
    out_mat.wait()
    out_norm.wait()
    out_max.wait()


def store_kernel(*refs):
    n = len(refs) // 2
    sem = refs[-1]
    copies = [pltpu.make_async_copy(refs[i], refs[n + i], sem.at[i]) for i in range(n)]
    for cp in copies:
        cp.start()
    for cp in copies:
        cp.wait()


def per_device(shape, *args):
    (hidden, mgain, wq, wk, wv, wo, wgates, bias, state, snorm, smax, wmix, fgain, routes, rw, eg, eu, ed, sg, su, sd) = args
    E, T = shape["ep"], shape["tp"]
    EX = 4 if E % 4 == 0 and E > 4 else 2
    EY, Z = E // EX, T // 2
    S, D = hidden.shape
    HN, HD = state.shape[1], state.shape[2]
    L, SW = eg.shape[0], sg.shape[1]
    W, KS, NS = D // T, D // E, E * L * ROOM
    f32, bf16 = jnp.float32, jnp.bfloat16
    V, dma = pltpu.VMEM, pltpu.SemaphoreType.DMA
    H = D // 2
    scratch = [
        V((S, D), bf16), V((1, D), f32), V((KS, 512), bf16), V((2, HN, D), bf16), V((2, HN), f32), V(state.shape, f32),
        V(snorm.shape, f32), V((HN, S), f32), V((2, wmix.shape[0], H), bf16), V((1, D), f32),
        V((2, routes.shape[0]), jnp.int32), V((2, S), f32), V((2, H, 4 * 128), bf16), V((2, L * 128, H), bf16),
        V((2, 2 * SW, H), bf16), V((2, SW, H), bf16),
        V((E, S, KS), bf16), V((E, S, KS), bf16), V((E, S, 512), bf16), V((E, S, 512), bf16),
        V((HN, 4, S, HD), f32), V((HN, S, HD), f32), V((S, HN * HD), bf16),
        V((Z, S, W), bf16), V((Z, S, W), bf16), V((Z, S, W), f32), V((Z, S, W), bf16), V((Z, S, W), bf16),
        V((S, W), bf16), V((2, Z, S, W), bf16), V((NS, H), bf16), V((2, NS, H), bf16), V((NS, H), bf16), V((S, H), bf16),
        V((NS, 512), f32), V((Z, NS, W), bf16), V((Z, NS, W), bf16), V((NS, H), bf16), V((NS, H), bf16),
        V((Z, S, W), bf16), V((Z, S, W), bf16), V((Z, S, W), f32), V((Z, S, W), bf16), V((Z, S, W), bf16),
        V(snorm.shape, f32), V((HN, S), f32),
        dma((10,)), dma((6,)), dma((12,)),
        dma((E,)), dma((1,)), dma((Z,)), dma((1,)), dma((Z,)), dma((1,)), dma((E,)), dma((1,)), dma((1,)), dma((Z,)),
        dma((Z,)), dma((1,)), dma((3,)),
    ]
    anywhere = pl.BlockSpec(memory_space=pl.ANY)
    operands = (
        hidden, mgain.reshape(1, D), wq, wk, wv, wo, jnp.swapaxes(wgates, 1, 2), bias, state, snorm, smax.T, wmix,
        fgain.reshape(1, D), routes.T, rw.T, eg, eu, ed, sg.T, su.T, sd,
    )
    results = ((S, W), bf16), (state.shape, f32), (snorm.shape, f32), ((HN, S), f32)
    inner = pl.pallas_call(
        functools.partial(layer_kernel, (EY, EX, Z, S, D, HD, L)),
        out_shape=tuple(V(*r) for r in results),
        in_specs=[anywhere] * len(operands),
        out_specs=(pl.BlockSpec(memory_space=V), anywhere, anywhere, anywhere),
        scratch_shapes=scratch,
        compiler_params=pltpu.CompilerParams(
            collective_id=0, has_side_effects=True, vmem_limit_bytes=48 * 1024 * 1024
        ),
        name="layer",
    )(*(pltpu.with_memory_space_constraint(a, pltpu.HBM) for a in operands))
    result, newmat, newnorm, newmax = pl.pallas_call(
        store_kernel,
        out_shape=tuple(jax.ShapeDtypeStruct(*r) for r in results),
        in_specs=[anywhere] * len(results),
        out_specs=(anywhere,) * len(results),
        scratch_shapes=[dma((len(results),))],
        compiler_params=pltpu.CompilerParams(vmem_limit_bytes=1024 * 1024),
        name="store",
    )(*(pltpu.with_memory_space_constraint(a, V) for a in inner))
    return result, newmat, newnorm, newmax.T


def solution(mesh):
    placed = (
        P("ep", None),
        P(),
        P("ep", "tp"),
        P("ep", "tp"),
        P("ep", "tp"),
        P("ep", "tp"),
        P(None, None, "tp"),
        P(None, "tp"),
        P("ep", "tp", None, None),
        P("ep", "tp", None),
        P("ep", "tp"),
        P("tp", None),
        P(),
        P(),
        P("ep", None),
        P("ep", None, "tp"),
        P("ep", None, "tp"),
        P("ep", "tp", None),
        P(None, "tp"),
        P(None, "tp"),
        P("tp", None),
    )
    return jax.shard_map(
        functools.partial(per_device, dict(mesh.shape)),
        mesh=mesh,
        in_specs=placed,
        out_specs=(P("ep", "tp"), P("ep", "tp", None, None), P("ep", "tp", None), P("ep", "tp")),
        check_vma=False,
    )
```

```python
import functools

import jax
import jax.numpy as jnp
from jax import lax
from jax.experimental import pallas as pl
from jax.experimental.pallas import tpu as pltpu
from jax.sharding import PartitionSpec as P

MESH = pl.DeviceIdType.MESH
NORM_EPS = 1e-06
ORDER_A = (1, 4, 3, 2)
ORDER_B = (1, 2, 4, 3)
ROOM = 4


def remote(src, dst, send_sem, recv_sem, dev):
    return pltpu.make_async_remote_copy(
        src_ref=src, dst_ref=dst, send_sem=send_sem, recv_sem=recv_sem, device_id=dev, device_id_type=MESH
    )


def wait_bytes(ref, sem):
    pltpu.make_async_copy(ref, ref, sem).wait()


def far_first(n):
    return sorted(range(1, n), key=lambda i: (-min(i, n - i), i))


def by_hops(ey, ex, order):
    def hops(i):
        dy, dx = i // ex, i % ex
        return min(dy, ey - dy) + min(dx, ex - dx)

    return [i for h in order for i in range(1, ey * ex) if hops(i) == h]


def near_first(n):
    return sorted(range(1, n), key=lambda i: (min(i, n - i), i))


def layer_kernel(
    cfg,
    hidden_h, mgain_h, wq_h, wk_h, wv_h, wo_h, wg_h, bias_h, state_h, snorm_h, smax_h, wmix_h, fgain_h,
    routes_h, rw_h, eg_h, eu_h, ed_h, sg_h, su_h, sd_h,
    result_o, newmat_o, newnorm_o, newmax_o,
    hid, mgain, wqkvo, wg, bias, state, snorm, smax, wmix, fgain, routes, rw, wcat, down, sgu, sdown,
    xn, ga, pt, qa, kvq, nums, gated, mixs, mixr, mixm, mixo, rz, so, st, disp, dx, xs, acc, sqs, po, pi, ret, rt,
    shs, shr, sho, fin, fz, nnew, mnew,
    lsem, bulk, sends, r1, r2, r3, r4, r5, r6, r7, r8, r9, r10, r11, r12, osem,
):
    EY, EX, Z, S, D, HD, L = cfg
    E, T = EY * EX, 2 * Z
    W = D // T
    f32, bf16 = jnp.float32, jnp.bfloat16
    e, t = lax.axis_index("ep"), lax.axis_index("tp")
    z, c = lax.div(t, 2), lax.rem(t, 2)
    o = 1 - c
    sib = (e, z * 2 + o)
    y, x = lax.div(e, EX), lax.rem(e, EX)
    s1, s2, s3, s4, s5, s6, s7, s8, s9, s10, s11, s12 = (sends.at[k] for k in range(12))

    def ep_peer(i):
        return lax.rem(y + lax.div(i, EX), EY) * EX + lax.rem(x + lax.rem(i, EX), EX)

    def ep_src(i):
        return lax.rem(y + EY - lax.div(i, EX), EY) * EX + lax.rem(x + EX - lax.rem(i, EX), EX)

    ypart = [lax.rem(y + k, EY) * EX for k in range(EY)]
    xpart = [lax.rem(x + k, EX) for k in range(EX)]
    peers = [None] + [ypart[i // EX] + xpart[i % EX] for i in range(1, E)]
    ep_far = by_hops(EY, EX, (4, 3, 2, 1))
    ep_sent = by_hops(EY, EX, ORDER_A)
    ep_done = by_hops(EY, EX, ORDER_B)

    def z_dev(zz):
        return (e, zz * 2 + c)

    def zp(i):
        return lax.rem(z + i, Z)

    def zs(i):
        return lax.rem(z + Z - i, Z)

    def col(zz, cc):
        return pl.ds(pl.multiple_of((zz * 2 + cc) * W, W), W)

    def half(zz):
        return pl.ds(pl.multiple_of(zz * W, W), W)

    def rows(g):
        return pl.ds(pl.multiple_of(g * L * ROOM, L * ROOM), L * ROOM)

    def each(first, n, step):
        def one(i, _):
            step(i)
            return 0

        lax.fori_loop(first, n, one, 0)

    barrier = pltpu.get_barrier_semaphore()

    def greet(dev):
        pl.semaphore_signal(barrier, inc=1, device_id=dev, device_id_type=MESH)

    loads = []

    def load(src, dst):
        cp = pltpu.make_async_copy(src, dst, lsem.at[len(loads)])
        cp.start()
        loads.append(cp)
        return cp

    ld_hid = load(hidden_h, hid)
    ld_mg = load(mgain_h, mgain)
    each(1, E, lambda i: greet((ep_peer(i), t)))
    for i in far_first(Z):
        greet(z_dev(zp(i)))
    greet(sib)
    for k, w in enumerate((wq_h, wk_h, wv_h, wo_h)):
        pltpu.make_async_copy(w, wqkvo.at[:, k * 128 : (k + 1) * 128], bulk.at[0]).start()

    ld_hid.wait()
    ld_mg.wait()
    KS = D // E
    sq = jnp.zeros((S, 128), f32)
    for k in range(D // 128):
        v = hid[:, k * 128 : (k + 1) * 128].astype(f32)
        sq = sq + v * v
    scale = lax.rsqrt(jnp.sum(sq, -1, keepdims=True) * (1.0 / D) + NORM_EPS)
    for k in range(E):
        v = hid[:, k * KS : (k + 1) * KS].astype(f32)
        xn[k] = (v * scale * mgain[:, k * KS : (k + 1) * KS]).astype(bf16)
    pl.semaphore_wait(barrier, E - 1 + Z - 1 + 1)

    def send_x(i):
        p = peers[i]
        remote(xn.at[p], ga.at[e], s1, r1.at[i], (p, t)).start()

    for i in ep_sent:
        send_x(i)

    ld_wg = load(wg_h, wg)
    ld_bi = load(bias_h, bias)
    ld_sm = load(smax_h, smax)
    ld_rt = load(routes_h, routes)
    ld_rw = load(rw_h, rw)
    ld_sn = load(snorm_h, snorm)
    ld_st = load(state_h, state)
    ld_fg = load(fgain_h, fgain)
    SW = sg_h.shape[0]

    def start_narrow(k):
        zz, cc = lax.div(k, 2), lax.rem(k, 2)
        cols = pl.ds(pl.multiple_of(k * W, W), W)
        pltpu.make_async_copy(wmix_h.at[:, cols], wmix.at[cc, :, half(zz)], bulk.at[1]).start()
        pltpu.make_async_copy(sg_h.at[:, cols], sgu.at[cc, 0:SW, half(zz)], bulk.at[2]).start()
        pltpu.make_async_copy(su_h.at[:, cols], sgu.at[cc, SW : 2 * SW, half(zz)], bulk.at[2]).start()
        pltpu.make_async_copy(sd_h.at[:, cols], sdown.at[cc, :, half(zz)], bulk.at[3]).start()

    def start_wide(k):
        zz, cc = lax.div(k, 2), lax.rem(k, 2)
        cols = pl.ds(pl.multiple_of(k * W, W), W)
        for j in range(L):
            for q, src in enumerate((eg_h, eu_h)):
                lanes = slice((2 * j + q) * 128, (2 * j + q + 1) * 128)
                pltpu.make_async_copy(src.at[j, cols, :], wcat.at[cc, half(zz), lanes], bulk.at[4]).start()
            pltpu.make_async_copy(
                ed_h.at[j, :, cols], down.at[cc, j * 128 : (j + 1) * 128, half(zz)], bulk.at[5]
            ).start()

    each(0, T, start_narrow)
    each(0, T, start_wide)

    wait_bytes(wqkvo, bulk.at[0])
    qa[0] = jnp.dot(xn[e], wqkvo[...], preferred_element_type=f32).astype(bf16)

    def project(i):
        g = ep_src(i)
        remote(xn.at[g], ga.at[g], s1, r1.at[i], (g, t)).wait_recv()
        pt[g] = jnp.dot(ga[g], wqkvo[...], preferred_element_type=f32).astype(bf16)
        remote(pt.at[g], qa.at[i], s2, r2.at[0], (g, t)).start()

    for i in ep_done:
        project(i)

    ld_wg.wait()
    ld_bi.wait()
    ld_sm.wait()
    ld_rt.wait()
    ld_rw.wait()
    HN = 2
    gsum = [[jnp.zeros((S, 128), f32) for _ in range(HN)] for _ in range(2)]
    for k in range(D // 128):
        v = xn[k * 128 // KS, :, (k * 128) % KS : (k * 128) % KS + 128].astype(f32)
        for g in range(2):
            w2 = wg[g, :, k * 128 : (k + 1) * 128].astype(f32)
            for h in range(HN):
                gsum[g][h] = gsum[g][h] + v * w2[h : h + 1, :]
    eye = lax.broadcasted_iota(jnp.int32, (S, S), 0) == lax.broadcasted_iota(jnp.int32, (S, S), 1)
    smax_v = smax[...]
    fws, iws = [], []
    for h in range(HN):
        gi = jnp.sum(gsum[0][h], -1, keepdims=True) + bias[0:1, h : h + 1]
        gf = jnp.sum(gsum[1][h], -1, keepdims=True) + bias[1:2, h : h + 1]
        old = jnp.sum(jnp.where(eye, smax_v[h : h + 1, :], 0.0), -1, keepdims=True)
        carried = jnp.minimum(gf, 0.0) - jnp.log(1.0 + jnp.exp(-jnp.abs(gf))) + old
        nm = jnp.maximum(carried, gi)
        fws.append(jnp.exp(carried - nm))
        iws.append(jnp.exp(gi - nm))
        mnew[h : h + 1, :] = jnp.sum(jnp.where(eye, nm, 0.0), 0, keepdims=True)
    out_max = pltpu.make_async_copy(mnew, newmax_o, osem.at[2])
    out_max.start()

    GR = routes_h.shape[1]
    sel = (
        lax.broadcasted_iota(jnp.int32, (S, GR), 1) == lax.broadcasted_iota(jnp.int32, (S, GR), 0) + e * S
    )
    all_routes = routes[...].astype(f32)
    sel_f = jnp.where(sel, 1.0, 0.0)
    r_col = [jnp.sum(sel_f * all_routes[j : j + 1, :], -1, keepdims=True) for j in range(2)]
    r_row = [jnp.sum(jnp.where(eye, r_col[j], 0.0), 0, keepdims=True) for j in range(2)]
    i0 = lax.broadcasted_iota(jnp.int32, (S, S), 0)
    i1 = lax.broadcasted_iota(jnp.int32, (S, S), 1)
    NS = E * L * ROOM
    slot_row, slot_col = [], []
    for j in range(2):
        same = jnp.where(r_col[0] == r_row[j], 1.0, 0.0) + jnp.where(r_col[1] == r_row[j], 1.0, 0.0)
        rank_row = jnp.sum(jnp.where(i0 < i1, same, 0.0), 0, keepdims=True)
        slot_row.append(r_row[j] * ROOM + rank_row)
        same = jnp.where(r_row[0] == r_col[j], 1.0, 0.0) + jnp.where(r_row[1] == r_col[j], 1.0, 0.0)
        rank_col = jnp.sum(jnp.where(i1 < i0, same, 0.0), -1, keepdims=True)
        slot_col.append(r_col[j] * ROOM + rank_col)
    slot_ids = lax.broadcasted_iota(jnp.int32, (NS, S), 0).astype(f32)
    chooser = jnp.where((slot_ids == slot_row[0]) | (slot_ids == slot_row[1]), 1.0, 0.0).astype(bf16)
    rw_v = rw[...]
    rw_col = [jnp.sum(jnp.where(eye, rw_v[j : j + 1, :], 0.0), -1, keepdims=True) for j in range(2)]
    lane_ids = lax.broadcasted_iota(jnp.int32, (S, NS), 1).astype(f32)
    wsel = jnp.where(lane_ids == slot_col[0], rw_col[0], 0.0) + jnp.where(lane_ids == slot_col[1], rw_col[1], 0.0)
    w_hi = wsel.astype(bf16)
    w_lo = (wsel - w_hi.astype(f32)).astype(bf16)
    w_both = jnp.concatenate([w_hi, w_lo], 0)

    ld_sn.wait()
    ld_st.wait()
    wait_bytes(qa.at[pl.ds(1, E - 1)], r2.at[0])
    roles = []
    for k in range(4):
        total = qa[0, :, k * 128 : (k + 1) * 128].astype(f32)
        for i in range(1, E):
            total = total + qa[i, :, k * 128 : (k + 1) * 128].astype(f32)
        roles.append(total.astype(bf16).astype(f32))

    for h in range(HN):
        hs = slice(h * HD, (h + 1) * HD)
        qh, kh, vh = roles[0][:, hs], roles[1][:, hs] * HD ** (-0.5), roles[2][:, hs]
        kvq[h, 0] = qh
        kvq[h, 1] = kh
        kvq[h, 2] = vh * iws[h]
        kvq[h, 3] = jnp.broadcast_to(fws[h], (S, HD))
    SB = 8

    def cell(b):
        at = pl.ds(pl.multiple_of(b * SB, SB), SB)
        for h in range(HN):
            new = (
                kvq[h, 3, at, :][:, None, :] * state[at, h]
                + kvq[h, 2, at, :][:, :, None] * kvq[h, 1, at, :][:, None, :]
            )
            state[at, h] = new
            nums[h, at, :] = jnp.sum(new * kvq[h, 0, at, :][:, None, :], -1)

    each(0, S // SB, cell)
    for h in range(HN):
        hs = slice(h * HD, (h + 1) * HD)
        nn = fws[h] * snorm[:, h, :] + iws[h] * kvq[h, 1]
        nnew[:, h, :] = nn
        den = jnp.maximum(jnp.abs(jnp.sum(nn * kvq[h, 0], -1, keepdims=True)), 1.0)
        gate = 1.0 / (1.0 + jnp.exp(-roles[3][:, hs]))
        gated[:, hs] = (gate * nums[h] / den).astype(bf16)

    wait_bytes(wmix, bulk.at[1])
    gv = gated[...]
    zorder = far_first(Z) + [0]
    theirs = jnp.dot(gv, wmix[o], preferred_element_type=f32)
    for zz in range(Z):
        mixs[zz] = theirs[:, zz * W : (zz + 1) * W].astype(bf16)
    for i in zorder:
        remote(mixs.at[zp(i)], mixr.at[zp(i)], s3, r3.at[i], sib).start()
    mine = jnp.dot(gv, wmix[c], preferred_element_type=f32)
    for zz in range(Z):
        mixm[zz] = mine[:, zz * W : (zz + 1) * W]
    own = None
    for i in zorder:
        zz = zp(i)
        remote(mixs.at[zz], mixr.at[zz], s3, r3.at[i], sib).wait_recv()
        both = mixm[zz] + mixr[zz].astype(f32)
        if i:
            mixo[i] = both.astype(bf16)
            remote(mixo.at[i], rz.at[i], s4, r4.at[0], z_dev(zz)).start()
        else:
            own = both
    out_mat = pltpu.make_async_copy(state, newmat_o, osem.at[0])
    out_mat.start()
    out_norm = pltpu.make_async_copy(nnew, newnorm_o, osem.at[1])
    out_norm.start()
    own = own + hid[:, pl.ds(pl.multiple_of(t * W, W), W)].astype(f32)
    wait_bytes(rz.at[pl.ds(1, Z - 1)], r4.at[0])
    for i in range(1, Z):
        own = own + rz[i].astype(f32)
    so[...] = own.astype(bf16)

    for i in far_first(Z):
        remote(so, st.at[c, z], s5, r5.at[i], z_dev(zp(i))).start()

    def dispatch(block, i):
        g = zs(i)
        disp[g] = jnp.dot(chooser, block, preferred_element_type=f32).astype(bf16)
        for k in ep_far:
            remote(disp.at[g, rows(peers[k])], dx.at[c, g, rows(e)], s7, r7.at[i], (peers[k], t)).start()
        pltpu.make_async_copy(disp.at[g, rows(e)], dx.at[c, g, rows(e)], r7.at[i]).start()

    dispatch(so[...], 0)
    remote(so, st.at[c, z], s6, r6.at[0], sib).start()
    st[c, z] = so[...]
    for i in near_first(Z):
        g = zs(i)
        remote(so, st.at[c, g], s5, r5.at[i], z_dev(g)).wait_recv()
        dispatch(st[c, g], i)
        remote(st.at[c, g], st.at[c, g], s6, r6.at[0], sib).start()

    ld_fg.wait()
    wait_bytes(sgu, bulk.at[2])
    wait_bytes(sdown, bulk.at[3])
    wait_bytes(st.at[o], r6.at[0])
    sq = jnp.zeros((S, W), f32)
    for cc in range(2):
        for zz in range(Z):
            v = st[cc, zz].astype(f32)
            sq = sq + v * v
    sscale = lax.rsqrt(jnp.sum(sq, -1, keepdims=True) * (1.0 / D) + NORM_EPS)
    pre = jnp.zeros((S, 2 * SW), f32)
    for cc in range(2):
        for zz in range(Z):
            cs = slice((zz * 2 + cc) * W, (zz * 2 + cc + 1) * W)
            xs[:, zz * W : (zz + 1) * W] = (st[cc, zz].astype(f32) * sscale * fgain[:, cs]).astype(bf16)
        pre = pre + lax.dot_general(xs[...], sgu[cc], (((1,), (1,)), ((), ())), preferred_element_type=f32)
    sgate, sup = pre[:, :SW], pre[:, SW:]
    shid = (sgate / (1.0 + jnp.exp(-sgate)) * sup).astype(bf16)
    theirs = jnp.dot(shid, sdown[o], preferred_element_type=f32)
    for zz in range(Z):
        shs[zz] = theirs[:, zz * W : (zz + 1) * W].astype(bf16)
    remote(shs, shr, s9, r9.at[0], sib).start()
    mine = jnp.dot(shid, sdown[c], preferred_element_type=f32)
    for zz in range(Z):
        sho[zz] = mine[:, zz * W : (zz + 1) * W]

    wait_bytes(wcat, bulk.at[4])
    acc[...] = jnp.zeros_like(acc)
    sqs[...] = jnp.zeros_like(sqs)

    def block_of(cc, g):
        v = dx[cc, g].astype(f32)
        scaled = (v * fgain[:, col(g, cc)]).astype(bf16)
        acc[...] += jnp.dot(scaled, wcat[cc, half(g), :], preferred_element_type=f32)
        v = v * v
        sqs[...] += sum(v[:, k * 128 : (k + 1) * 128] for k in range(W // 128))

    arrivals = [0] + near_first(Z)
    BEHIND = min(2, Z)
    for k in range(Z + BEHIND):
        if k < Z:
            i = arrivals[k]
            g = zs(i)
            wait_bytes(dx.at[c, g], r7.at[i])
            remote(dx.at[c, g], dx.at[c, g], s8, r8.at[i], sib).start()
            block_of(c, g)
        if k >= BEHIND:
            i = arrivals[k - BEHIND]
            g = zs(i)
            remote(dx.at[c, g], dx.at[o, g], s8, r8.at[i], sib).wait_recv()
            block_of(o, g)
    sq = sqs[...]
    escale = lax.rsqrt(jnp.sum(sq, -1, keepdims=True) * (1.0 / D) + NORM_EPS)
    expert_of = lax.rem(lax.div(lax.broadcasted_iota(jnp.int32, (NS, 128), 0), ROOM), L)
    hids = []
    for j in range(L):
        gv = acc[:, 2 * j * 128 : (2 * j + 1) * 128] * escale
        uv = acc[:, (2 * j + 1) * 128 : (2 * j + 2) * 128] * escale
        hids.append(jnp.where(expert_of == j, gv / (1.0 + jnp.exp(-gv)) * uv, 0.0).astype(bf16))
    hcat = jnp.concatenate(hids, 1)

    wait_bytes(down, bulk.at[5])
    LAG = min(3, Z)

    def down_theirs(i):
        zz = zp(i)
        po[i] = jnp.dot(hcat, down[o, :, half(zz)], preferred_element_type=f32).astype(bf16)
        remote(po.at[i], pi.at[i], s10, r10.at[i], sib).start()

    def down_mine(i):
        zz = zp(i)
        part = jnp.dot(hcat, down[c, :, half(zz)], preferred_element_type=f32)
        remote(po.at[i], pi.at[i], s10, r10.at[i], sib).wait_recv()
        ret[i] = (part + pi[i].astype(f32)).astype(bf16)

        for k in ep_far:
            p = peers[k]
            remote(ret.at[i, rows(p)], rt.at[i, rows(e)], s11, r11.at[i], (p, t)).start()

        pltpu.make_async_copy(ret.at[i, rows(e)], rt.at[i, rows(e)], r11.at[i]).start()

    for k in range(Z + LAG):
        if k < Z:
            down_theirs(zorder[k])
        if k >= LAG:
            down_mine(zorder[k - LAG])

    remote(shs, shr, s9, r9.at[0], sib).wait_recv()
    own = None
    for i in zorder:
        zz = zp(i)
        wait_bytes(rt.at[i], r11.at[i])
        two = jnp.dot(w_both, rt[i], preferred_element_type=f32)
        both = two[:S] + two[S:] + sho[zz] + shr[zz].astype(f32)
        if i:
            fin[i] = both.astype(bf16)
            remote(fin.at[i], fz.at[i], s12, r12.at[0], z_dev(zz)).start()
        else:
            own = both
    own = own + so[...].astype(f32)
    wait_bytes(fz.at[pl.ds(1, Z - 1)], r12.at[0])
    for i in range(1, Z):
        own = own + fz[i].astype(f32)
    result_o[...] = own.astype(bf16)

    wait_bytes(xn.at[pl.ds(1, E - 1)], s1)
    wait_bytes(pt.at[pl.ds(1, E - 1)], s2)
    wait_bytes(mixs, s3)
    wait_bytes(mixo.at[pl.ds(1, Z - 1)], s4)
    wait_bytes(mixo.at[pl.ds(1, Z - 1)], s5)
    wait_bytes(mixs, s6)
    wait_bytes(disp.at[:, pl.ds(0, NS - L * ROOM)], s7)
    wait_bytes(disp, s8)
    wait_bytes(shs, s9)
    wait_bytes(po, s10)
    wait_bytes(ret.at[:, pl.ds(0, NS - L * ROOM)], s11)
    wait_bytes(fin.at[pl.ds(1, Z - 1)], s12)
    out_mat.wait()
    out_norm.wait()
    out_max.wait()


def store_kernel(*refs):
    n = len(refs) // 2
    sem = refs[-1]
    copies = [pltpu.make_async_copy(refs[i], refs[n + i], sem.at[i]) for i in range(n)]
    for cp in copies:
        cp.start()
    for cp in copies:
        cp.wait()


def per_device(shape, *args):
    (hidden, mgain, wq, wk, wv, wo, wgates, bias, state, snorm, smax, wmix, fgain, routes, rw, eg, eu, ed, sg, su, sd) = args
    E, T = shape["ep"], shape["tp"]
    EX = 4 if E % 4 == 0 and E > 4 else 2
    EY, Z = E // EX, T // 2
    S, D = hidden.shape
    HN, HD = state.shape[1], state.shape[2]
    L, SW = eg.shape[0], sg.shape[1]
    W, KS, NS = D // T, D // E, E * L * ROOM
    f32, bf16 = jnp.float32, jnp.bfloat16
    V, dma = pltpu.VMEM, pltpu.SemaphoreType.DMA
    H = D // 2
    scratch = [
        V((S, D), bf16), V((1, D), f32), V((KS, 512), bf16), V((2, HN, D), bf16), V((2, HN), f32), V(state.shape, f32),
        V(snorm.shape, f32), V((HN, S), f32), V((2, wmix.shape[0], H), bf16), V((1, D), f32),
        V((2, routes.shape[0]), jnp.int32), V((2, S), f32), V((2, H, 4 * 128), bf16), V((2, L * 128, H), bf16),
        V((2, 2 * SW, H), bf16), V((2, SW, H), bf16),
        V((E, S, KS), bf16), V((E, S, KS), bf16), V((E, S, 512), bf16), V((E, S, 512), bf16),
        V((HN, 4, S, HD), f32), V((HN, S, HD), f32), V((S, HN * HD), bf16),
        V((Z, S, W), bf16), V((Z, S, W), bf16), V((Z, S, W), f32), V((Z, S, W), bf16), V((Z, S, W), bf16),
        V((S, W), bf16), V((2, Z, S, W), bf16), V((Z, NS, W), bf16), V((2, Z, NS, W), bf16), V((S, H), bf16), V((NS, 512), f32), V((NS, 128), f32),
        V((Z, NS, W), bf16), V((Z, NS, W), bf16), V((Z, NS, W), bf16), V((Z, NS, W), bf16),
        V((Z, S, W), bf16), V((Z, S, W), bf16), V((Z, S, W), f32), V((Z, S, W), bf16), V((Z, S, W), bf16),
        V(snorm.shape, f32), V((HN, S), f32),
        dma((10,)), dma((6,)), dma((12,)),
        dma((E,)), dma((1,)), dma((Z,)), dma((1,)), dma((Z,)), dma((1,)), dma((Z,)), dma((Z,)), dma((1,)), dma((Z,)),
        dma((Z,)), dma((1,)), dma((3,)),
    ]
    anywhere = pl.BlockSpec(memory_space=pl.ANY)
    operands = (
        hidden, mgain.reshape(1, D), wq, wk, wv, wo, jnp.swapaxes(wgates, 1, 2), bias, state, snorm, smax.T, wmix,
        fgain.reshape(1, D), routes.T, rw.T, eg, eu, ed, sg.T, su.T, sd,
    )
    results = ((S, W), bf16), (state.shape, f32), (snorm.shape, f32), ((HN, S), f32)
    inner = pl.pallas_call(
        functools.partial(layer_kernel, (EY, EX, Z, S, D, HD, L)),
        out_shape=tuple(V(*r) for r in results),
        in_specs=[anywhere] * len(operands),
        out_specs=(pl.BlockSpec(memory_space=V), anywhere, anywhere, anywhere),
        scratch_shapes=scratch,
        compiler_params=pltpu.CompilerParams(
            collective_id=0, has_side_effects=True, vmem_limit_bytes=48 * 1024 * 1024
        ),
        name="layer",
    )(*(pltpu.with_memory_space_constraint(a, pltpu.HBM) for a in operands))
    result, newmat, newnorm, newmax = pl.pallas_call(
        store_kernel,
        out_shape=tuple(jax.ShapeDtypeStruct(*r) for r in results),
        in_specs=[anywhere] * len(results),
        out_specs=(anywhere,) * len(results),
        scratch_shapes=[dma((len(results),))],
        compiler_params=pltpu.CompilerParams(vmem_limit_bytes=1024 * 1024),
        name="store",
    )(*(pltpu.with_memory_space_constraint(a, V) for a in inner))
    return result, newmat, newnorm, newmax.T


def solution(mesh):
    placed = (
        P("ep", None),
        P(),
        P("ep", "tp"),
        P("ep", "tp"),
        P("ep", "tp"),
        P("ep", "tp"),
        P(None, None, "tp"),
        P(None, "tp"),
        P("ep", "tp", None, None),
        P("ep", "tp", None),
        P("ep", "tp"),
        P("tp", None),
        P(),
        P(),
        P("ep", None),
        P("ep", None, "tp"),
        P("ep", None, "tp"),
        P("ep", "tp", None),
        P(None, "tp"),
        P(None, "tp"),
        P("tp", None),
    )
    return jax.shard_map(
        functools.partial(per_device, dict(mesh.shape)),
        mesh=mesh,
        in_specs=placed,
        out_specs=(P("ep", "tp"), P("ep", "tp", None, None), P("ep", "tp", None), P("ep", "tp")),
        check_vma=False,
    )
```

```python
import functools

import jax
import jax.numpy as jnp
from jax import lax
from jax.experimental import pallas as pl
from jax.experimental.pallas import tpu as pltpu
from jax.sharding import PartitionSpec as P

MESH = pl.DeviceIdType.MESH
NORM_EPS = 1e-06
CLASSES = (1,), (2,), (4, 3)
PARTS = 4
CAP = 3
PAIRS = 4
SENT = 3


def remote(src, dst, send_sem, recv_sem, dev):
    return pltpu.make_async_remote_copy(
        src_ref=src, dst_ref=dst, send_sem=send_sem, recv_sem=recv_sem, device_id=dev, device_id_type=MESH
    )


def wait_bytes(ref, sem):
    pltpu.make_async_copy(ref, ref, sem).wait()


def far_first(n):
    return sorted(range(1, n), key=lambda i: (-min(i, n - i), i))


def by_hops(ey, ex, order):
    def hops(i):
        dy, dx = i // ex, i % ex
        return min(dy, ey - dy) + min(dx, ex - dx)

    return [i for h in order for i in range(1, ey * ex) if hops(i) == h]


def near_first(n):
    return sorted(range(1, n), key=lambda i: (min(i, n - i), i))


def layer_kernel(
    cfg,
    hidden_h, mgain_h, wq_h, wk_h, wv_h, wo_h, wg_h, bias_h, state_h, snorm_h, smax_h, wmix_h, fgain_h,
    routes_h, rw_h, eg_h, eu_h, ed_h, sg_h, su_h, sd_h,
    result_o, newmat_o, newnorm_o, newmax_o,
    hid, mgain, wqkvo, wg, bias, state, snorm, smax, wmix, fgain, routes, rw, wcat, down, sgu, sdown,
    xn, ga, pt, qa, kvq, nums, gated, mixs, mixr, mixm, mixo, rz, so, st, disp, dx, xs, acc, sqs, po, pi, ret, rt,
    shs, shr, sho, fin, fz, nnew, mnew,
    lsem, bulk, sends, r1, r2, r3, r4, r5, r6, r7, r8, r9, r10, r11, r12, osem,
):
    EY, EX, Z, S, D, HD, L = cfg
    E, T = EY * EX, 2 * Z
    W = D // T
    f32, bf16 = jnp.float32, jnp.bfloat16
    e, t = lax.axis_index("ep"), lax.axis_index("tp")
    z, c = lax.div(t, 2), lax.rem(t, 2)
    o = 1 - c
    sib = (e, z * 2 + o)
    y, x = lax.div(e, EX), lax.rem(e, EX)
    s1, s2, s3, s4, s5, s6, s7, s8, s9, s10, s11, s12 = (sends.at[k] for k in range(12))

    def ep_peer(i):
        return lax.rem(y + lax.div(i, EX), EY) * EX + lax.rem(x + lax.rem(i, EX), EX)

    def ep_src(i):
        return lax.rem(y + EY - lax.div(i, EX), EY) * EX + lax.rem(x + EX - lax.rem(i, EX), EX)

    ypart = [lax.rem(y + k, EY) * EX for k in range(EY)]
    xpart = [lax.rem(x + k, EX) for k in range(EX)]
    peers = [None] + [ypart[i // EX] + xpart[i % EX] for i in range(1, E)]
    ep_far = by_hops(EY, EX, (4, 3, 2, 1))
    classes = [k for k in (by_hops(EY, EX, hops) for hops in CLASSES) if k]
    starts = [1 + sum(len(k) for k in classes[:n]) for n in range(len(classes))]

    def z_dev(zz):
        return (e, zz * 2 + c)

    def zp(i):
        return lax.rem(z + i, Z)

    def zs(i):
        return lax.rem(z + Z - i, Z)

    def col(zz, cc):
        return pl.ds(pl.multiple_of((zz * 2 + cc) * W, W), W)

    def half(zz):
        return pl.ds(pl.multiple_of(zz * W, W), W)

    used = pl.ds(0, SENT)
    GROUP = 2 * PAIRS

    def each(first, n, step):
        def one(i, _):
            step(i)
            return 0

        lax.fori_loop(first, n, one, 0)

    barrier = pltpu.get_barrier_semaphore()

    def greet(dev):
        pl.semaphore_signal(barrier, inc=1, device_id=dev, device_id_type=MESH)

    loads = []

    def load(src, dst):
        cp = pltpu.make_async_copy(src, dst, lsem.at[len(loads)])
        cp.start()
        loads.append(cp)
        return cp

    ld_hid = load(hidden_h, hid)
    ld_mg = load(mgain_h, mgain)
    each(1, E, lambda i: greet((ep_peer(i), t)))
    for i in far_first(Z):
        greet(z_dev(zp(i)))
    greet(sib)
    for k, w in enumerate((wq_h, wk_h, wv_h, wo_h)):
        pltpu.make_async_copy(w, wqkvo.at[:, k * 128 : (k + 1) * 128], bulk.at[0]).start()

    ld_hid.wait()
    ld_mg.wait()
    KS = D // E
    sq = jnp.zeros((S, 128), f32)
    for k in range(D // 128):
        v = hid[:, k * 128 : (k + 1) * 128].astype(f32)
        sq = sq + v * v
    scale = lax.rsqrt(jnp.sum(sq, -1, keepdims=True) * (1.0 / D) + NORM_EPS)
    for k in range(E):
        v = hid[:, k * KS : (k + 1) * KS].astype(f32)
        xn[k] = (v * scale * mgain[:, k * KS : (k + 1) * KS]).astype(bf16)
    pl.semaphore_wait(barrier, E - 1 + Z - 1 + 1)

    for n, (first, members) in enumerate(zip(starts, classes)):
        for k, i in enumerate(members):
            remote(xn.at[peers[i]], ga.at[first + k], s1, r1.at[n], (peers[i], t)).start()

    ld_wg = load(wg_h, wg)
    ld_bi = load(bias_h, bias)
    ld_sm = load(smax_h, smax)
    ld_rt = load(routes_h, routes)
    ld_rw = load(rw_h, rw)
    ld_sn = load(snorm_h, snorm)
    ld_st = load(state_h, state)
    ld_fg = load(fgain_h, fgain)
    SW = sg_h.shape[0]

    def start_narrow(k):
        zz, cc = lax.div(k, 2), lax.rem(k, 2)
        cols = pl.ds(pl.multiple_of(k * W, W), W)
        pltpu.make_async_copy(wmix_h.at[:, cols], wmix.at[cc, :, half(zz)], bulk.at[1]).start()
        pltpu.make_async_copy(sg_h.at[:, cols], sgu.at[cc, 0:SW, half(zz)], bulk.at[2]).start()
        pltpu.make_async_copy(su_h.at[:, cols], sgu.at[cc, SW : 2 * SW, half(zz)], bulk.at[2]).start()
        pltpu.make_async_copy(sd_h.at[:, cols], sdown.at[cc, :, half(zz)], bulk.at[3]).start()

    def start_wide(k):
        zz, cc = lax.div(k, 2), lax.rem(k, 2)
        cols = pl.ds(pl.multiple_of(k * W, W), W)
        for j in range(L):
            for q, src in enumerate((eg_h, eu_h)):
                lanes = slice((2 * j + q) * 128, (2 * j + q + 1) * 128)
                pltpu.make_async_copy(src.at[j, cols, :], wcat.at[cc, half(zz), lanes], bulk.at[4]).start()
            pltpu.make_async_copy(
                ed_h.at[j, :, cols], down.at[cc, j * 128 : (j + 1) * 128, half(zz)], bulk.at[5]
            ).start()

    each(0, T, start_narrow)
    each(0, T, start_wide)

    dx[...] = jnp.zeros_like(dx)
    rt[...] = jnp.zeros_like(rt)

    wait_bytes(wqkvo, bulk.at[0])
    qa[0] = jnp.dot(xn[e], wqkvo[...], preferred_element_type=f32).astype(bf16)

    for n, (first, members) in enumerate(zip(starts, classes)):
        many = len(members)
        wait_bytes(ga.at[pl.ds(first, many)], r1.at[n])
        parts = jnp.dot(ga[first : first + many].reshape(many * S, KS), wqkvo[...], preferred_element_type=f32)
        pt[first : first + many] = parts.astype(bf16).reshape(many, S, 4 * 128)
        for k, i in enumerate(members):
            g = ep_src(i)
            remote(pt.at[first + k], qa.at[first + k], s2, r2.at[n], (g, t)).start()

    ld_wg.wait()
    ld_bi.wait()
    ld_sm.wait()
    ld_rt.wait()
    ld_rw.wait()
    HN = 2
    gsum = [[jnp.zeros((S, 128), f32) for _ in range(HN)] for _ in range(2)]
    for k in range(D // 128):
        v = xn[k * 128 // KS, :, (k * 128) % KS : (k * 128) % KS + 128].astype(f32)
        for g in range(2):
            w2 = wg[g, :, k * 128 : (k + 1) * 128].astype(f32)
            for h in range(HN):
                gsum[g][h] = gsum[g][h] + v * w2[h : h + 1, :]
    eye = lax.broadcasted_iota(jnp.int32, (S, S), 0) == lax.broadcasted_iota(jnp.int32, (S, S), 1)
    smax_v = smax[...]
    fws, iws = [], []
    for h in range(HN):
        gi = jnp.sum(gsum[0][h], -1, keepdims=True) + bias[0:1, h : h + 1]
        gf = jnp.sum(gsum[1][h], -1, keepdims=True) + bias[1:2, h : h + 1]
        old = jnp.sum(jnp.where(eye, smax_v[h : h + 1, :], 0.0), -1, keepdims=True)
        carried = jnp.minimum(gf, 0.0) - jnp.log(1.0 + jnp.exp(-jnp.abs(gf))) + old
        nm = jnp.maximum(carried, gi)
        fws.append(jnp.exp(carried - nm))
        iws.append(jnp.exp(gi - nm))
        mnew[h : h + 1, :] = jnp.sum(jnp.where(eye, nm, 0.0), 0, keepdims=True)
    out_max = pltpu.make_async_copy(mnew, newmax_o, osem.at[2])
    out_max.start()

    GR = routes_h.shape[1]
    sel = (
        lax.broadcasted_iota(jnp.int32, (S, GR), 1) == lax.broadcasted_iota(jnp.int32, (S, GR), 0) + e * S
    )
    all_routes = routes[...].astype(f32)
    sel_f = jnp.where(sel, 1.0, 0.0)
    r_col = [jnp.sum(sel_f * all_routes[j : j + 1, :], -1, keepdims=True) for j in range(2)]
    r_row = [jnp.sum(jnp.where(eye, r_col[j], 0.0), 0, keepdims=True) for j in range(2)]
    i0 = lax.broadcasted_iota(jnp.int32, (S, S), 0)
    i1 = lax.broadcasted_iota(jnp.int32, (S, S), 1)
    NS = E * GROUP

    def first_slot(expert):
        ids = expert.astype(jnp.int32)
        dev = lax.div(ids, L)
        return (dev * GROUP + (ids - dev * L) * CAP).astype(f32)

    slot_row, slot_col = [], []
    for j in range(2):
        same = jnp.where(r_col[0] == r_row[j], 1.0, 0.0) + jnp.where(r_col[1] == r_row[j], 1.0, 0.0)
        rank_row = jnp.sum(jnp.where(i0 < i1, same, 0.0), 0, keepdims=True)
        slot_row.append(first_slot(r_row[j]) + rank_row)
        same = jnp.where(r_row[0] == r_col[j], 1.0, 0.0) + jnp.where(r_row[1] == r_col[j], 1.0, 0.0)
        rank_col = jnp.sum(jnp.where(i1 < i0, same, 0.0), -1, keepdims=True)
        slot_col.append(first_slot(r_col[j]) + rank_col)
    slot_ids = lax.broadcasted_iota(jnp.int32, (NS, S), 0).astype(f32)
    chooser = jnp.where((slot_ids == slot_row[0]) | (slot_ids == slot_row[1]), 1.0, 0.0).astype(bf16)
    rw_v = rw[...]
    rw_col = [jnp.sum(jnp.where(eye, rw_v[j : j + 1, :], 0.0), -1, keepdims=True) for j in range(2)]
    lane_ids = lax.broadcasted_iota(jnp.int32, (S, NS), 1).astype(f32)
    wsel = jnp.where(lane_ids == slot_col[0], rw_col[0], 0.0) + jnp.where(lane_ids == slot_col[1], rw_col[1], 0.0)
    w_hi = wsel.astype(bf16)
    w_lo = (wsel - w_hi.astype(f32)).astype(bf16)
    w_both = jnp.concatenate([w_hi, w_lo], 0)

    ld_sn.wait()
    ld_st.wait()
    roles = [qa[0, :, k * 128 : (k + 1) * 128].astype(f32) for k in range(4)]
    for n, (first, members) in enumerate(zip(starts, classes)):
        wait_bytes(qa.at[pl.ds(first, len(members))], r2.at[n])
        for k in range(4):
            for i in range(first, first + len(members)):
                roles[k] = roles[k] + qa[i, :, k * 128 : (k + 1) * 128].astype(f32)
    roles = [r.astype(bf16).astype(f32) for r in roles]

    for h in range(HN):
        hs = slice(h * HD, (h + 1) * HD)
        qh, kh, vh = roles[0][:, hs], roles[1][:, hs] * HD ** (-0.5), roles[2][:, hs]
        kvq[h, 0] = qh
        kvq[h, 1] = kh
        kvq[h, 2] = vh * iws[h]
        kvq[h, 3] = jnp.broadcast_to(fws[h], (S, HD))
    SB = 8

    def seqs(b):
        return pl.ds(pl.multiple_of(b * SB, SB), SB)

    def read(b):
        for h in range(HN):
            nums[h, seqs(b), :] = jnp.sum(state[seqs(b), h] * kvq[h, 0, seqs(b), :][:, None, :], -1)

    each(0, S // SB, read)
    for h in range(HN):
        hs = slice(h * HD, (h + 1) * HD)
        nn = fws[h] * snorm[:, h, :] + iws[h] * kvq[h, 1]
        nnew[:, h, :] = nn
        den = jnp.maximum(jnp.abs(jnp.sum(nn * kvq[h, 0], -1, keepdims=True)), 1.0)
        gate = 1.0 / (1.0 + jnp.exp(-roles[3][:, hs]))
        num = fws[h] * nums[h] + kvq[h, 2] * jnp.sum(kvq[h, 1] * kvq[h, 0], -1, keepdims=True)
        gated[:, hs] = (gate * num / den).astype(bf16)

    wait_bytes(wmix, bulk.at[1])
    gv = gated[...]
    zorder = far_first(Z) + [0]
    theirs = jnp.dot(gv, wmix[o], preferred_element_type=f32)
    for zz in range(Z):
        mixs[zz] = theirs[:, zz * W : (zz + 1) * W].astype(bf16)
    remote(mixs, mixr, s3, r3.at[0], sib).start()
    mine = jnp.dot(gv, wmix[c], preferred_element_type=f32)
    for zz in range(Z):
        mixm[zz] = mine[:, zz * W : (zz + 1) * W]
    own = None
    remote(mixs, mixr, s3, r3.at[0], sib).wait_recv()
    for i in zorder:
        zz = zp(i)
        both = mixm[zz] + mixr[zz].astype(f32)
        if i:
            mixo[i] = both.astype(bf16)
            remote(mixo.at[i], rz.at[i], s4, r4.at[0], z_dev(zz)).start()
        else:
            own = both

    def update(b):
        for h in range(HN):
            state[seqs(b), h] = (
                kvq[h, 3, seqs(b), :][:, None, :] * state[seqs(b), h]
                + kvq[h, 2, seqs(b), :][:, :, None] * kvq[h, 1, seqs(b), :][:, None, :]
            )

    each(0, S // SB, update)
    out_mat = pltpu.make_async_copy(state, newmat_o, osem.at[0])
    out_mat.start()
    out_norm = pltpu.make_async_copy(nnew, newnorm_o, osem.at[1])
    out_norm.start()
    own = own + hid[:, pl.ds(pl.multiple_of(t * W, W), W)].astype(f32)
    wait_bytes(rz.at[pl.ds(1, Z - 1)], r4.at[0])
    for i in range(1, Z):
        own = own + rz[i].astype(f32)
    so[...] = own.astype(bf16)

    for i in far_first(Z):
        remote(so, st.at[c, z], s5, r5.at[i], z_dev(zp(i))).start()

    def dispatch(block, i):
        g = zs(i)
        disp[g] = jnp.dot(chooser, block, preferred_element_type=f32).astype(bf16).reshape(E, PAIRS, 2, W)
        for k in ep_far:
            remote(disp.at[g, peers[k], used], dx.at[c, g, e, used], s7, r7.at[i], (peers[k], t)).start()
        pltpu.make_async_copy(disp.at[g, e, used], dx.at[c, g, e, used], r7.at[i]).start()

    dispatch(so[...], 0)
    remote(so, st.at[c, z], s6, r6.at[0], sib).start()
    st[c, z] = so[...]
    for i in near_first(Z):
        g = zs(i)
        remote(so, st.at[c, g], s5, r5.at[i], z_dev(g)).wait_recv()
        dispatch(st[c, g], i)
        remote(st.at[c, g], st.at[c, g], s6, r6.at[0], sib).start()

    ld_fg.wait()
    wait_bytes(sgu, bulk.at[2])
    wait_bytes(sdown, bulk.at[3])
    wait_bytes(st.at[o], r6.at[0])
    sq = jnp.zeros((S, W), f32)
    for cc in range(2):
        for zz in range(Z):
            v = st[cc, zz].astype(f32)
            sq = sq + v * v
    sscale = lax.rsqrt(jnp.sum(sq, -1, keepdims=True) * (1.0 / D) + NORM_EPS)
    pre = jnp.zeros((S, 2 * SW), f32)
    for cc in range(2):
        for zz in range(Z):
            cs = slice((zz * 2 + cc) * W, (zz * 2 + cc + 1) * W)
            xs[:, zz * W : (zz + 1) * W] = (st[cc, zz].astype(f32) * sscale * fgain[:, cs]).astype(bf16)
        pre = pre + lax.dot_general(xs[...], sgu[cc], (((1,), (1,)), ((), ())), preferred_element_type=f32)
    sgate, sup = pre[:, :SW], pre[:, SW:]
    shid = (sgate / (1.0 + jnp.exp(-sgate)) * sup).astype(bf16)
    theirs = jnp.dot(shid, sdown[o], preferred_element_type=f32)
    for zz in range(Z):
        shs[zz] = theirs[:, zz * W : (zz + 1) * W].astype(bf16)
    remote(shs, shr, s9, r9.at[0], sib).start()
    mine = jnp.dot(shid, sdown[c], preferred_element_type=f32)
    for zz in range(Z):
        sho[zz] = mine[:, zz * W : (zz + 1) * W]

    wait_bytes(wcat, bulk.at[4])
    acc[...] = jnp.zeros_like(acc)
    sqs[...] = jnp.zeros_like(sqs)

    def block_of(cc, g):
        v = dx[cc, g].reshape(NS, W).astype(f32)
        scaled = (v * fgain[:, col(g, cc)]).astype(bf16)
        acc[...] += jnp.dot(scaled, wcat[cc, half(g), :], preferred_element_type=f32)
        v = v * v
        sqs[...] += sum(v[:, k * 128 : (k + 1) * 128] for k in range(W // 128))

    arrivals = [0] + near_first(Z)
    BEHIND = min(2, Z)
    for k in range(Z + BEHIND):
        if k < Z:
            i = arrivals[k]
            g = zs(i)
            wait_bytes(dx.at[c, g, :, used], r7.at[i])
            remote(dx.at[c, g], dx.at[c, g], s8, r8.at[i], sib).start()
            block_of(c, g)
        if k >= BEHIND:
            i = arrivals[k - BEHIND]
            g = zs(i)
            remote(dx.at[c, g], dx.at[o, g], s8, r8.at[i], sib).wait_recv()
            block_of(o, g)
    sq = sqs[...]
    escale = lax.rsqrt(jnp.sum(sq, -1, keepdims=True) * (1.0 / D) + NORM_EPS)
    expert_of = lax.div(lax.rem(lax.broadcasted_iota(jnp.int32, (NS, 128), 0), GROUP), CAP)
    hids = []
    for j in range(L):
        gv = acc[:, 2 * j * 128 : (2 * j + 1) * 128] * escale
        uv = acc[:, (2 * j + 1) * 128 : (2 * j + 2) * 128] * escale
        hids.append(jnp.where(expert_of == j, gv / (1.0 + jnp.exp(-gv)) * uv, 0.0).astype(bf16))
    hcat = jnp.concatenate(hids, 1)

    wait_bytes(down, bulk.at[5])
    LAG = min(3, Z)

    def down_theirs(i):
        zz = zp(i)
        po[i] = jnp.dot(hcat, down[o, :, half(zz)], preferred_element_type=f32).astype(bf16)
        remote(po.at[i], pi.at[i], s10, r10.at[i], sib).start()

    def down_mine(i):
        zz = zp(i)
        part = jnp.dot(hcat, down[c, :, half(zz)], preferred_element_type=f32)
        remote(po.at[i], pi.at[i], s10, r10.at[i], sib).wait_recv()
        ret[i] = (part + pi[i].astype(f32)).astype(bf16).reshape(E, PAIRS, 2, W)

        for k in ep_far:
            p = peers[k]
            remote(ret.at[i, p, used], rt.at[i, e, used], s11, r11.at[i], (p, t)).start()

        pltpu.make_async_copy(ret.at[i, e, used], rt.at[i, e, used], r11.at[i]).start()

    for k in range(Z + LAG):
        if k < Z:
            down_theirs(zorder[k])
        if k >= LAG:
            down_mine(zorder[k - LAG])

    remote(shs, shr, s9, r9.at[0], sib).wait_recv()
    own = None
    for i in zorder:
        zz = zp(i)
        wait_bytes(rt.at[i, :, used], r11.at[i])
        two = jnp.dot(w_both, rt[i].reshape(NS, W), preferred_element_type=f32)
        both = two[:S] + two[S:] + sho[zz] + shr[zz].astype(f32)
        if i:
            fin[i] = both.astype(bf16)
            remote(fin.at[i], fz.at[i], s12, r12.at[0], z_dev(zz)).start()
        else:
            own = both
    own = own + so[...].astype(f32)
    wait_bytes(fz.at[pl.ds(1, Z - 1)], r12.at[0])
    for i in range(1, Z):
        own = own + fz[i].astype(f32)
    result_o[...] = own.astype(bf16)

    wait_bytes(xn.at[pl.ds(1, E - 1)], s1)
    wait_bytes(pt.at[pl.ds(1, E - 1)], s2)
    wait_bytes(mixs, s3)
    wait_bytes(mixo.at[pl.ds(1, Z - 1)], s4)
    wait_bytes(mixo.at[pl.ds(1, Z - 1)], s5)
    wait_bytes(mixs, s6)
    wait_bytes(disp.at[:, pl.ds(0, E - 1), used], s7)
    wait_bytes(disp, s8)
    wait_bytes(shs, s9)
    wait_bytes(po, s10)
    wait_bytes(ret.at[:, pl.ds(0, E - 1), used], s11)
    wait_bytes(fin.at[pl.ds(1, Z - 1)], s12)
    out_mat.wait()
    out_norm.wait()
    out_max.wait()


def store_kernel(*refs):
    n = len(refs) // 2
    sem = refs[-1]
    copies = [pltpu.make_async_copy(refs[i], refs[n + i], sem.at[i]) for i in range(n) if i != 1]
    part = refs[1].shape[0] // PARTS
    for k in range(PARTS):
        some = pl.ds(k * part, part)
        copies.append(pltpu.make_async_copy(refs[1].at[some], refs[n + 1].at[some], sem.at[n + k]))
    for cp in copies:
        cp.start()
    for cp in copies:
        cp.wait()


def per_device(shape, *args):
    (hidden, mgain, wq, wk, wv, wo, wgates, bias, state, snorm, smax, wmix, fgain, routes, rw, eg, eu, ed, sg, su, sd) = args
    E, T = shape["ep"], shape["tp"]
    EX = 4 if E % 4 == 0 and E > 4 else 2
    EY, Z = E // EX, T // 2
    S, D = hidden.shape
    HN, HD = state.shape[1], state.shape[2]
    L, SW = eg.shape[0], sg.shape[1]
    W, KS, NS = D // T, D // E, E * 2 * PAIRS
    f32, bf16 = jnp.float32, jnp.bfloat16
    V, dma = pltpu.VMEM, pltpu.SemaphoreType.DMA
    H = D // 2
    scratch = [
        V((S, D), bf16), V((1, D), f32), V((KS, 512), bf16), V((2, HN, D), bf16), V((2, HN), f32), V(state.shape, f32),
        V(snorm.shape, f32), V((HN, S), f32), V((2, wmix.shape[0], H), bf16), V((1, D), f32),
        V((2, routes.shape[0]), jnp.int32), V((2, S), f32), V((2, H, 4 * 128), bf16), V((2, L * 128, H), bf16),
        V((2, 2 * SW, H), bf16), V((2, SW, H), bf16),
        V((E, S, KS), bf16), V((E, S, KS), bf16), V((E, S, 512), bf16), V((E, S, 512), bf16),
        V((HN, 4, S, HD), f32), V((HN, S, HD), f32), V((S, HN * HD), bf16),
        V((Z, S, W), bf16), V((Z, S, W), bf16), V((Z, S, W), f32), V((Z, S, W), bf16), V((Z, S, W), bf16),
        V((S, W), bf16), V((2, Z, S, W), bf16), V((Z, E, PAIRS, 2, W), bf16), V((2, Z, E, PAIRS, 2, W), bf16), V((S, H), bf16), V((NS, 512), f32), V((NS, 128), f32),
        V((Z, NS, W), bf16), V((Z, NS, W), bf16), V((Z, E, PAIRS, 2, W), bf16), V((Z, E, PAIRS, 2, W), bf16),
        V((Z, S, W), bf16), V((Z, S, W), bf16), V((Z, S, W), f32), V((Z, S, W), bf16), V((Z, S, W), bf16),
        V(snorm.shape, f32), V((HN, S), f32),
        dma((10,)), dma((6,)), dma((12,)),
        dma((3,)), dma((3,)), dma((1,)), dma((1,)), dma((Z,)), dma((1,)), dma((Z,)), dma((Z,)), dma((1,)), dma((Z,)),
        dma((Z,)), dma((1,)), dma((3,)),
    ]
    anywhere = pl.BlockSpec(memory_space=pl.ANY)
    operands = (
        hidden, mgain.reshape(1, D), wq, wk, wv, wo, jnp.swapaxes(wgates, 1, 2), bias, state, snorm, smax.T, wmix,
        fgain.reshape(1, D), routes.T, rw.T, eg, eu, ed, sg.T, su.T, sd,
    )
    results = ((S, W), bf16), (state.shape, f32), (snorm.shape, f32), ((HN, S), f32)
    inner = pl.pallas_call(
        functools.partial(layer_kernel, (EY, EX, Z, S, D, HD, L)),
        out_shape=tuple(V(*r) for r in results),
        in_specs=[anywhere] * len(operands),
        out_specs=(pl.BlockSpec(memory_space=V), anywhere, anywhere, anywhere),
        scratch_shapes=scratch,
        compiler_params=pltpu.CompilerParams(
            collective_id=0, has_side_effects=True, vmem_limit_bytes=48 * 1024 * 1024
        ),
        name="layer",
    )(*(pltpu.with_memory_space_constraint(a, pltpu.HBM) for a in operands))
    result, newmat, newnorm, newmax = pl.pallas_call(
        store_kernel,
        out_shape=tuple(jax.ShapeDtypeStruct(*r) for r in results),
        in_specs=[anywhere] * len(results),
        out_specs=(anywhere,) * len(results),
        scratch_shapes=[dma((len(results) + PARTS,))],
        compiler_params=pltpu.CompilerParams(vmem_limit_bytes=1024 * 1024),
        name="store",
    )(*(pltpu.with_memory_space_constraint(a, V) for a in inner))
    return result, newmat, newnorm, newmax.T


def solution(mesh):
    placed = (
        P("ep", None),
        P(),
        P("ep", "tp"),
        P("ep", "tp"),
        P("ep", "tp"),
        P("ep", "tp"),
        P(None, None, "tp"),
        P(None, "tp"),
        P("ep", "tp", None, None),
        P("ep", "tp", None),
        P("ep", "tp"),
        P("tp", None),
        P(),
        P(),
        P("ep", None),
        P("ep", None, "tp"),
        P("ep", None, "tp"),
        P("ep", "tp", None),
        P(None, "tp"),
        P(None, "tp"),
        P("tp", None),
    )
    return jax.shard_map(
        functools.partial(per_device, dict(mesh.shape)),
        mesh=mesh,
        in_specs=placed,
        out_specs=(P("ep", "tp"), P("ep", "tp", None, None), P("ep", "tp", None), P("ep", "tp")),
        check_vma=False,
    )
```

```python
import functools

import jax
import jax.numpy as jnp
from jax import lax
from jax.experimental import pallas as pl
from jax.experimental.pallas import tpu as pltpu
from jax.sharding import PartitionSpec as P

MESH = pl.DeviceIdType.MESH
NORM_EPS = 1e-06
CLASSES = (1,), (2,), (4, 3)
PARTS = 4
CAP = 3
PAIRS = 4
SENT = 3


def remote(src, dst, send_sem, recv_sem, dev):
    return pltpu.make_async_remote_copy(
        src_ref=src, dst_ref=dst, send_sem=send_sem, recv_sem=recv_sem, device_id=dev, device_id_type=MESH
    )


def wait_bytes(ref, sem):
    pltpu.make_async_copy(ref, ref, sem).wait()


def far_first(n):
    return sorted(range(1, n), key=lambda i: (-min(i, n - i), i))


def by_hops(ey, ex, order):
    def hops(i):
        dy, dx = i // ex, i % ex
        return min(dy, ey - dy) + min(dx, ex - dx)

    return [i for h in order for i in range(1, ey * ex) if hops(i) == h]


def near_first(n):
    return sorted(range(1, n), key=lambda i: (min(i, n - i), i))


def layer_kernel(
    cfg,
    hidden_h, mgain_h, wq_h, wk_h, wv_h, wo_h, wg_h, bias_h, state_h, snorm_h, smax_h, wmix_h, fgain_h,
    routes_h, rw_h, eg_h, eu_h, ed_h, sg_h, su_h, sd_h,
    result_o, newmat_o, newnorm_o, newmax_o,
    hid, mgain, wqkvo, wg, bias, state, snorm, smax, wmix, fgain, routes, rw, wcat, down, sgu, sdown,
    xn, ga, pt, qa, kvq, nums, gated, mixs, mixr, mixm, mixo, rz, so, st, disp, dx, xs, acc, sqs, po, pi, ret, rt,
    shs, shr, sho, fin, fz, nnew, mnew,
    lsem, bulk, sends, r1, r2, r3, r4, r5, r6, r7, r8, r9, r10, r11, r12, osem,
):
    EY, EX, Z, S, D, HD, L = cfg
    E, T = EY * EX, 2 * Z
    W = D // T
    f32, bf16 = jnp.float32, jnp.bfloat16
    e, t = lax.axis_index("ep"), lax.axis_index("tp")
    z, c = lax.div(t, 2), lax.rem(t, 2)
    o = 1 - c
    sib = (e, z * 2 + o)
    y, x = lax.div(e, EX), lax.rem(e, EX)
    s1, s2, s3, s4, s5, s6, s7, s8, s9, s10, s11, s12 = (sends.at[k] for k in range(12))

    def ep_peer(i):
        return lax.rem(y + lax.div(i, EX), EY) * EX + lax.rem(x + lax.rem(i, EX), EX)

    def ep_src(i):
        return lax.rem(y + EY - lax.div(i, EX), EY) * EX + lax.rem(x + EX - lax.rem(i, EX), EX)

    ypart = [lax.rem(y + k, EY) * EX for k in range(EY)]
    xpart = [lax.rem(x + k, EX) for k in range(EX)]
    peers = [None] + [ypart[i // EX] + xpart[i % EX] for i in range(1, E)]
    ep_far = by_hops(EY, EX, (4, 3, 2, 1))
    classes = [k for k in (by_hops(EY, EX, hops) for hops in CLASSES) if k]
    starts = [1 + sum(len(k) for k in classes[:n]) for n in range(len(classes))]

    def z_dev(zz):
        return (e, zz * 2 + c)

    def zp(i):
        return lax.rem(z + i, Z)

    def zs(i):
        return lax.rem(z + Z - i, Z)

    def col(zz, cc):
        return pl.ds(pl.multiple_of((zz * 2 + cc) * W, W), W)

    def half(zz):
        return pl.ds(pl.multiple_of(zz * W, W), W)

    used = pl.ds(0, SENT)
    GROUP = 2 * PAIRS

    def each(first, n, step):
        def one(i, _):
            step(i)
            return 0

        lax.fori_loop(first, n, one, 0)

    barrier = pltpu.get_barrier_semaphore()

    def greet(dev):
        pl.semaphore_signal(barrier, inc=1, device_id=dev, device_id_type=MESH)

    loads = []

    def load(src, dst):
        cp = pltpu.make_async_copy(src, dst, lsem.at[len(loads)])
        cp.start()
        loads.append(cp)
        return cp

    ld_hid = load(hidden_h, hid)
    ld_mg = load(mgain_h, mgain)
    each(1, E, lambda i: greet((ep_peer(i), t)))
    for i in far_first(Z):
        greet(z_dev(zp(i)))
    greet(sib)
    for k, w in enumerate((wq_h, wk_h, wv_h, wo_h)):
        pltpu.make_async_copy(w, wqkvo.at[:, k * 128 : (k + 1) * 128], bulk.at[0]).start()

    ld_hid.wait()
    ld_mg.wait()
    KS = D // E
    sq = jnp.zeros((S, 128), f32)
    for k in range(D // 128):
        v = hid[:, k * 128 : (k + 1) * 128].astype(f32)
        sq = sq + v * v
    scale = lax.rsqrt(jnp.sum(sq, -1, keepdims=True) * (1.0 / D) + NORM_EPS)
    for k in range(E):
        v = hid[:, k * KS : (k + 1) * KS].astype(f32)
        xn[k] = (v * scale * mgain[:, k * KS : (k + 1) * KS]).astype(bf16)
    pl.semaphore_wait(barrier, E - 1 + Z - 1 + 1)

    for n, (first, members) in enumerate(zip(starts, classes)):
        for k, i in enumerate(members):
            remote(xn.at[peers[i]], ga.at[first + k], s1, r1.at[n], (peers[i], t)).start()

    ld_wg = load(wg_h, wg)
    ld_bi = load(bias_h, bias)
    ld_sm = load(smax_h, smax)
    ld_rt = load(routes_h, routes)
    ld_rw = load(rw_h, rw)
    ld_sn = load(snorm_h, snorm)
    ld_st = load(state_h, state)
    ld_fg = load(fgain_h, fgain)
    SW = sg_h.shape[0]

    def start_narrow(k):
        zz, cc = lax.div(k, 2), lax.rem(k, 2)
        cols = pl.ds(pl.multiple_of(k * W, W), W)
        pltpu.make_async_copy(wmix_h.at[:, cols], wmix.at[cc, :, half(zz)], bulk.at[1]).start()
        pltpu.make_async_copy(sg_h.at[:, cols], sgu.at[cc, 0:SW, half(zz)], bulk.at[2]).start()
        pltpu.make_async_copy(su_h.at[:, cols], sgu.at[cc, SW : 2 * SW, half(zz)], bulk.at[2]).start()
        pltpu.make_async_copy(sd_h.at[:, cols], sdown.at[cc, :, half(zz)], bulk.at[3]).start()

    def start_wide(k):
        zz, cc = lax.div(k, 2), lax.rem(k, 2)
        cols = pl.ds(pl.multiple_of(k * W, W), W)
        for j in range(L):
            for q, src in enumerate((eg_h, eu_h)):
                lanes = slice((2 * j + q) * 128, (2 * j + q + 1) * 128)
                pltpu.make_async_copy(src.at[j, cols, :], wcat.at[cc, half(zz), lanes], bulk.at[4]).start()
            pltpu.make_async_copy(
                ed_h.at[j, :, cols], down.at[cc, j * 128 : (j + 1) * 128, half(zz)], bulk.at[5]
            ).start()

    each(0, T, start_narrow)
    each(0, T, start_wide)

    dx[...] = jnp.zeros_like(dx)
    rt[...] = jnp.zeros_like(rt)

    wait_bytes(wqkvo, bulk.at[0])
    qa[0] = jnp.dot(xn[e], wqkvo[...], preferred_element_type=f32).astype(bf16)

    for n, (first, members) in enumerate(zip(starts, classes)):
        many = len(members)
        wait_bytes(ga.at[pl.ds(first, many)], r1.at[n])
        parts = jnp.dot(ga[first : first + many].reshape(many * S, KS), wqkvo[...], preferred_element_type=f32)
        pt[first : first + many] = parts.astype(bf16).reshape(many, S, 4 * 128)
        for k, i in enumerate(members):
            g = ep_src(i)
            remote(pt.at[first + k], qa.at[first + k], s2, r2.at[n], (g, t)).start()

    ld_wg.wait()
    ld_bi.wait()
    ld_sm.wait()
    ld_rt.wait()
    ld_rw.wait()
    HN = 2
    gsum = [[jnp.zeros((S, 128), f32) for _ in range(HN)] for _ in range(2)]
    for k in range(D // 128):
        v = xn[k * 128 // KS, :, (k * 128) % KS : (k * 128) % KS + 128].astype(f32)
        for g in range(2):
            w2 = wg[g, :, k * 128 : (k + 1) * 128].astype(f32)
            for h in range(HN):
                gsum[g][h] = gsum[g][h] + v * w2[h : h + 1, :]
    eye = lax.broadcasted_iota(jnp.int32, (S, S), 0) == lax.broadcasted_iota(jnp.int32, (S, S), 1)
    smax_v = smax[...]
    fws, iws = [], []
    for h in range(HN):
        gi = jnp.sum(gsum[0][h], -1, keepdims=True) + bias[0:1, h : h + 1]
        gf = jnp.sum(gsum[1][h], -1, keepdims=True) + bias[1:2, h : h + 1]
        old = jnp.sum(jnp.where(eye, smax_v[h : h + 1, :], 0.0), -1, keepdims=True)
        carried = jnp.minimum(gf, 0.0) - jnp.log(1.0 + jnp.exp(-jnp.abs(gf))) + old
        nm = jnp.maximum(carried, gi)
        fws.append(jnp.exp(carried - nm))
        iws.append(jnp.exp(gi - nm))
        mnew[h : h + 1, :] = jnp.sum(jnp.where(eye, nm, 0.0), 0, keepdims=True)
    out_max = pltpu.make_async_copy(mnew, newmax_o, osem.at[2])
    out_max.start()

    GR = routes_h.shape[1]
    sel = (
        lax.broadcasted_iota(jnp.int32, (S, GR), 1) == lax.broadcasted_iota(jnp.int32, (S, GR), 0) + e * S
    )
    all_routes = routes[...].astype(f32)
    sel_f = jnp.where(sel, 1.0, 0.0)
    r_col = [jnp.sum(sel_f * all_routes[j : j + 1, :], -1, keepdims=True) for j in range(2)]
    r_row = [jnp.sum(jnp.where(eye, r_col[j], 0.0), 0, keepdims=True) for j in range(2)]
    i0 = lax.broadcasted_iota(jnp.int32, (S, S), 0)
    i1 = lax.broadcasted_iota(jnp.int32, (S, S), 1)
    NS = E * GROUP

    def first_slot(expert):
        ids = expert.astype(jnp.int32)
        dev = lax.div(ids, L)
        return (dev * GROUP + (ids - dev * L) * CAP).astype(f32)

    slot_row, slot_col = [], []
    for j in range(2):
        same = jnp.where(r_col[0] == r_row[j], 1.0, 0.0) + jnp.where(r_col[1] == r_row[j], 1.0, 0.0)
        rank_row = jnp.sum(jnp.where(i0 < i1, same, 0.0), 0, keepdims=True)
        slot_row.append(first_slot(r_row[j]) + rank_row)
        same = jnp.where(r_row[0] == r_col[j], 1.0, 0.0) + jnp.where(r_row[1] == r_col[j], 1.0, 0.0)
        rank_col = jnp.sum(jnp.where(i1 < i0, same, 0.0), -1, keepdims=True)
        slot_col.append(first_slot(r_col[j]) + rank_col)
    slot_ids = lax.broadcasted_iota(jnp.int32, (NS, S), 0).astype(f32)
    chooser = jnp.where((slot_ids == slot_row[0]) | (slot_ids == slot_row[1]), 1.0, 0.0).astype(bf16)
    rw_v = rw[...]
    rw_col = [jnp.sum(jnp.where(eye, rw_v[j : j + 1, :], 0.0), -1, keepdims=True) for j in range(2)]
    lane_ids = lax.broadcasted_iota(jnp.int32, (S, NS), 1).astype(f32)
    wsel = jnp.where(lane_ids == slot_col[0], rw_col[0], 0.0) + jnp.where(lane_ids == slot_col[1], rw_col[1], 0.0)
    w_hi = wsel.astype(bf16)
    w_lo = (wsel - w_hi.astype(f32)).astype(bf16)
    w_both = jnp.concatenate([w_hi, w_lo], 0)

    ld_sn.wait()
    ld_st.wait()
    roles = [qa[0, :, k * 128 : (k + 1) * 128].astype(f32) for k in range(4)]
    for n, (first, members) in enumerate(zip(starts, classes)):
        wait_bytes(qa.at[pl.ds(first, len(members))], r2.at[n])
        for k in range(4):
            for i in range(first, first + len(members)):
                roles[k] = roles[k] + qa[i, :, k * 128 : (k + 1) * 128].astype(f32)
    roles = [r.astype(bf16).astype(f32) for r in roles]

    for h in range(HN):
        hs = slice(h * HD, (h + 1) * HD)
        qh, kh, vh = roles[0][:, hs], roles[1][:, hs] * HD ** (-0.5), roles[2][:, hs]
        kvq[h, 0] = qh
        kvq[h, 1] = kh
        kvq[h, 2] = vh * iws[h]
        kvq[h, 3] = jnp.broadcast_to(fws[h], (S, HD))
    SB = 8

    def seqs(b):
        return pl.ds(pl.multiple_of(b * SB, SB), SB)

    def read(b):
        for h in range(HN):
            nums[h, seqs(b), :] = jnp.sum(state[seqs(b), h] * kvq[h, 0, seqs(b), :][:, None, :], -1)

    each(0, S // SB, read)
    for h in range(HN):
        hs = slice(h * HD, (h + 1) * HD)
        nn = fws[h] * snorm[:, h, :] + iws[h] * kvq[h, 1]
        nnew[:, h, :] = nn
        den = jnp.maximum(jnp.abs(jnp.sum(nn * kvq[h, 0], -1, keepdims=True)), 1.0)
        gate = 1.0 / (1.0 + jnp.exp(-roles[3][:, hs]))
        num = fws[h] * nums[h] + kvq[h, 2] * jnp.sum(kvq[h, 1] * kvq[h, 0], -1, keepdims=True)
        gated[:, hs] = (gate * num / den).astype(bf16)

    wait_bytes(wmix, bulk.at[1])
    gv = gated[...]
    zorder = far_first(Z) + [0]
    theirs = jnp.dot(gv, wmix[o], preferred_element_type=f32)
    for zz in range(Z):
        mixs[zz] = theirs[:, zz * W : (zz + 1) * W].astype(bf16)
    remote(mixs, mixr, s3, r3.at[0], sib).start()
    mine = jnp.dot(gv, wmix[c], preferred_element_type=f32)
    for zz in range(Z):
        mixm[zz] = mine[:, zz * W : (zz + 1) * W]
    own = None
    remote(mixs, mixr, s3, r3.at[0], sib).wait_recv()
    for i in zorder:
        zz = zp(i)
        both = mixm[zz] + mixr[zz].astype(f32)
        if i:
            mixo[i] = both.astype(bf16)
            remote(mixo.at[i], rz.at[i], s4, r4.at[0], z_dev(zz)).start()
        else:
            own = both

    def update(b):
        for h in range(HN):
            state[seqs(b), h] = (
                kvq[h, 3, seqs(b), :][:, None, :] * state[seqs(b), h]
                + kvq[h, 2, seqs(b), :][:, :, None] * kvq[h, 1, seqs(b), :][:, None, :]
            )

    each(0, S // SB, update)
    out_mat = pltpu.make_async_copy(state, newmat_o, osem.at[0])
    out_mat.start()
    out_norm = pltpu.make_async_copy(nnew, newnorm_o, osem.at[1])
    out_norm.start()
    own = own + hid[:, pl.ds(pl.multiple_of(t * W, W), W)].astype(f32)
    wait_bytes(rz.at[pl.ds(1, Z - 1)], r4.at[0])
    for i in range(1, Z):
        own = own + rz[i].astype(f32)
    so[...] = own.astype(bf16)

    for i in far_first(Z):
        remote(so, st.at[c, z], s5, r5.at[i], z_dev(zp(i))).start()

    def dispatch(block, i):
        g = zs(i)
        disp[g] = jnp.dot(chooser, block, preferred_element_type=f32).astype(bf16).reshape(E, PAIRS, 2, W)
        for k in ep_far:
            remote(disp.at[g, peers[k], used], dx.at[c, g, e, used], s7, r7.at[i], (peers[k], t)).start()
        pltpu.make_async_copy(disp.at[g, e, used], dx.at[c, g, e, used], r7.at[i]).start()

    dispatch(so[...], 0)
    remote(so, st.at[c, z], s6, r6.at[0], sib).start()
    st[c, z] = so[...]
    for i in near_first(Z):
        g = zs(i)
        remote(so, st.at[c, g], s5, r5.at[i], z_dev(g)).wait_recv()
        dispatch(st[c, g], i)
        remote(st.at[c, g], st.at[c, g], s6, r6.at[0], sib).start()

    ld_fg.wait()
    wait_bytes(sgu, bulk.at[2])
    wait_bytes(sdown, bulk.at[3])
    wait_bytes(st.at[o], r6.at[0])
    sq = jnp.zeros((S, W), f32)
    for cc in range(2):
        for zz in range(Z):
            v = st[cc, zz].astype(f32)
            sq = sq + v * v
    sscale = lax.rsqrt(jnp.sum(sq, -1, keepdims=True) * (1.0 / D) + NORM_EPS)
    pre = jnp.zeros((S, 2 * SW), f32)
    for cc in range(2):
        for zz in range(Z):
            cs = slice((zz * 2 + cc) * W, (zz * 2 + cc + 1) * W)
            xs[:, zz * W : (zz + 1) * W] = (st[cc, zz].astype(f32) * sscale * fgain[:, cs]).astype(bf16)
        pre = pre + lax.dot_general(xs[...], sgu[cc], (((1,), (1,)), ((), ())), preferred_element_type=f32)
    sgate, sup = pre[:, :SW], pre[:, SW:]
    shid = (sgate / (1.0 + jnp.exp(-sgate)) * sup).astype(bf16)
    theirs = jnp.dot(shid, sdown[o], preferred_element_type=f32)
    for zz in range(Z):
        shs[zz] = theirs[:, zz * W : (zz + 1) * W].astype(bf16)
    remote(shs, shr, s9, r9.at[0], sib).start()
    mine = jnp.dot(shid, sdown[c], preferred_element_type=f32)
    for zz in range(Z):
        sho[zz] = mine[:, zz * W : (zz + 1) * W]

    wait_bytes(wcat, bulk.at[4])
    acc[...] = jnp.zeros_like(acc)
    sqs[...] = jnp.zeros_like(sqs)

    def block_of(cc, g):
        v = dx[cc, g].reshape(NS, W).astype(f32)
        scaled = (v * fgain[:, col(g, cc)]).astype(bf16)
        acc[...] += jnp.dot(scaled, wcat[cc, half(g), :], preferred_element_type=f32)
        v = v * v
        sqs[...] += sum(v[:, k * 128 : (k + 1) * 128] for k in range(W // 128))

    arrivals = [0] + near_first(Z)
    BEHIND = min(2, Z)
    for k in range(Z + BEHIND):
        if k < Z:
            i = arrivals[k]
            g = zs(i)
            wait_bytes(dx.at[c, g, :, used], r7.at[i])
            remote(dx.at[c, g, :, used], dx.at[c, g, :, used], s8, r8.at[i], sib).start()
            block_of(c, g)
        if k >= BEHIND:
            i = arrivals[k - BEHIND]
            g = zs(i)
            wait_bytes(dx.at[o, g, :, used], r8.at[i])
            block_of(o, g)
    sq = sqs[...]
    escale = lax.rsqrt(jnp.sum(sq, -1, keepdims=True) * (1.0 / D) + NORM_EPS)
    expert_of = lax.div(lax.rem(lax.broadcasted_iota(jnp.int32, (NS, 128), 0), GROUP), CAP)
    hids = []
    for j in range(L):
        gv = acc[:, 2 * j * 128 : (2 * j + 1) * 128] * escale
        uv = acc[:, (2 * j + 1) * 128 : (2 * j + 2) * 128] * escale
        hids.append(jnp.where(expert_of == j, gv / (1.0 + jnp.exp(-gv)) * uv, 0.0).astype(bf16))
    hcat = jnp.concatenate(hids, 1)

    wait_bytes(down, bulk.at[5])
    LAG = min(3, Z)

    def down_theirs(i):
        zz = zp(i)
        po[i] = jnp.dot(hcat, down[o, :, half(zz)], preferred_element_type=f32).astype(bf16)
        remote(po.at[i], pi.at[i], s10, r10.at[i], sib).start()

    def down_mine(i):
        zz = zp(i)
        part = jnp.dot(hcat, down[c, :, half(zz)], preferred_element_type=f32)
        remote(po.at[i], pi.at[i], s10, r10.at[i], sib).wait_recv()
        ret[i] = (part + pi[i].astype(f32)).astype(bf16).reshape(E, PAIRS, 2, W)

        for k in ep_far:
            p = peers[k]
            remote(ret.at[i, p, used], rt.at[i, e, used], s11, r11.at[i], (p, t)).start()

        pltpu.make_async_copy(ret.at[i, e, used], rt.at[i, e, used], r11.at[i]).start()

    for k in range(Z + LAG):
        if k < Z:
            down_theirs(zorder[k])
        if k >= LAG:
            down_mine(zorder[k - LAG])

    remote(shs, shr, s9, r9.at[0], sib).wait_recv()
    own = None
    for i in zorder:
        zz = zp(i)
        wait_bytes(rt.at[i, :, used], r11.at[i])
        two = jnp.dot(w_both, rt[i].reshape(NS, W), preferred_element_type=f32)
        both = two[:S] + two[S:] + sho[zz] + shr[zz].astype(f32)
        if i:
            fin[i] = both.astype(bf16)
            remote(fin.at[i], fz.at[i], s12, r12.at[0], z_dev(zz)).start()
        else:
            own = both
    own = own + so[...].astype(f32)
    wait_bytes(fz.at[pl.ds(1, Z - 1)], r12.at[0])
    for i in range(1, Z):
        own = own + fz[i].astype(f32)
    result_o[...] = own.astype(bf16)

    wait_bytes(xn.at[pl.ds(1, E - 1)], s1)
    wait_bytes(pt.at[pl.ds(1, E - 1)], s2)
    wait_bytes(mixs, s3)
    wait_bytes(mixo.at[pl.ds(1, Z - 1)], s4)
    wait_bytes(mixo.at[pl.ds(1, Z - 1)], s5)
    wait_bytes(mixs, s6)
    wait_bytes(disp.at[:, pl.ds(0, E - 1), used], s7)
    wait_bytes(disp.at[:, :, used], s8)
    wait_bytes(shs, s9)
    wait_bytes(po, s10)
    wait_bytes(ret.at[:, pl.ds(0, E - 1), used], s11)
    wait_bytes(fin.at[pl.ds(1, Z - 1)], s12)
    out_mat.wait()
    out_norm.wait()
    out_max.wait()


def store_kernel(*refs):
    n = len(refs) // 2
    sem = refs[-1]
    copies = [pltpu.make_async_copy(refs[i], refs[n + i], sem.at[i]) for i in range(n) if i != 1]
    part = refs[1].shape[0] // PARTS
    for k in range(PARTS):
        some = pl.ds(k * part, part)
        copies.append(pltpu.make_async_copy(refs[1].at[some], refs[n + 1].at[some], sem.at[n + k]))
    for cp in copies:
        cp.start()
    for cp in copies:
        cp.wait()


def per_device(shape, *args):
    (hidden, mgain, wq, wk, wv, wo, wgates, bias, state, snorm, smax, wmix, fgain, routes, rw, eg, eu, ed, sg, su, sd) = args
    E, T = shape["ep"], shape["tp"]
    EX = 4 if E % 4 == 0 and E > 4 else 2
    EY, Z = E // EX, T // 2
    S, D = hidden.shape
    HN, HD = state.shape[1], state.shape[2]
    L, SW = eg.shape[0], sg.shape[1]
    W, KS, NS = D // T, D // E, E * 2 * PAIRS
    f32, bf16 = jnp.float32, jnp.bfloat16
    V, dma = pltpu.VMEM, pltpu.SemaphoreType.DMA
    H = D // 2
    scratch = [
        V((S, D), bf16), V((1, D), f32), V((KS, 512), bf16), V((2, HN, D), bf16), V((2, HN), f32), V(state.shape, f32),
        V(snorm.shape, f32), V((HN, S), f32), V((2, wmix.shape[0], H), bf16), V((1, D), f32),
        V((2, routes.shape[0]), jnp.int32), V((2, S), f32), V((2, H, 4 * 128), bf16), V((2, L * 128, H), bf16),
        V((2, 2 * SW, H), bf16), V((2, SW, H), bf16),
        V((E, S, KS), bf16), V((E, S, KS), bf16), V((E, S, 512), bf16), V((E, S, 512), bf16),
        V((HN, 4, S, HD), f32), V((HN, S, HD), f32), V((S, HN * HD), bf16),
        V((Z, S, W), bf16), V((Z, S, W), bf16), V((Z, S, W), f32), V((Z, S, W), bf16), V((Z, S, W), bf16),
        V((S, W), bf16), V((2, Z, S, W), bf16), V((Z, E, PAIRS, 2, W), bf16), V((2, Z, E, PAIRS, 2, W), bf16), V((S, H), bf16), V((NS, 512), f32), V((NS, 128), f32),
        V((Z, NS, W), bf16), V((Z, NS, W), bf16), V((Z, E, PAIRS, 2, W), bf16), V((Z, E, PAIRS, 2, W), bf16),
        V((Z, S, W), bf16), V((Z, S, W), bf16), V((Z, S, W), f32), V((Z, S, W), bf16), V((Z, S, W), bf16),
        V(snorm.shape, f32), V((HN, S), f32),
        dma((10,)), dma((6,)), dma((12,)),
        dma((3,)), dma((3,)), dma((1,)), dma((1,)), dma((Z,)), dma((1,)), dma((Z,)), dma((Z,)), dma((1,)), dma((Z,)),
        dma((Z,)), dma((1,)), dma((3,)),
    ]
    anywhere = pl.BlockSpec(memory_space=pl.ANY)
    operands = (
        hidden, mgain.reshape(1, D), wq, wk, wv, wo, jnp.swapaxes(wgates, 1, 2), bias, state, snorm, smax.T, wmix,
        fgain.reshape(1, D), routes.T, rw.T, eg, eu, ed, sg.T, su.T, sd,
    )
    results = ((S, W), bf16), (state.shape, f32), (snorm.shape, f32), ((HN, S), f32)
    inner = pl.pallas_call(
        functools.partial(layer_kernel, (EY, EX, Z, S, D, HD, L)),
        out_shape=tuple(V(*r) for r in results),
        in_specs=[anywhere] * len(operands),
        out_specs=(pl.BlockSpec(memory_space=V), anywhere, anywhere, anywhere),
        scratch_shapes=scratch,
        compiler_params=pltpu.CompilerParams(
            collective_id=0, has_side_effects=True, vmem_limit_bytes=48 * 1024 * 1024
        ),
        name="layer",
    )(*(pltpu.with_memory_space_constraint(a, pltpu.HBM) for a in operands))
    result, newmat, newnorm, newmax = pl.pallas_call(
        store_kernel,
        out_shape=tuple(jax.ShapeDtypeStruct(*r) for r in results),
        in_specs=[anywhere] * len(results),
        out_specs=(anywhere,) * len(results),
        scratch_shapes=[dma((len(results) + PARTS,))],
        compiler_params=pltpu.CompilerParams(vmem_limit_bytes=1024 * 1024),
        name="store",
    )(*(pltpu.with_memory_space_constraint(a, V) for a in inner))
    return result, newmat, newnorm, newmax.T


def solution(mesh):
    placed = (
        P("ep", None),
        P(),
        P("ep", "tp"),
        P("ep", "tp"),
        P("ep", "tp"),
        P("ep", "tp"),
        P(None, None, "tp"),
        P(None, "tp"),
        P("ep", "tp", None, None),
        P("ep", "tp", None),
        P("ep", "tp"),
        P("tp", None),
        P(),
        P(),
        P("ep", None),
        P("ep", None, "tp"),
        P("ep", None, "tp"),
        P("ep", "tp", None),
        P(None, "tp"),
        P(None, "tp"),
        P("tp", None),
    )
    return jax.shard_map(
        functools.partial(per_device, dict(mesh.shape)),
        mesh=mesh,
        in_specs=placed,
        out_specs=(P("ep", "tp"), P("ep", "tp", None, None), P("ep", "tp", None), P("ep", "tp")),
        check_vma=False,
    )
```
